32 devices in a mesh: sp: 8 (over z, y), tp: 4 (over x, core).
Axes of the slice: x: 2, y: 2, z: 4, core: 2. Of those that a mesh axis runs over, the one named last changes fastest.
Arguments:
- tokens: bfloat16 [8192, 2048], P('sp'), may hold values from -6 to 6
- in_gain: float32 [2048], replicated, may hold values from 0.1 to 1.9
- w_query: bfloat16 [2048, 1024], P(None, 'tp'), may hold values from -0.125 to 0.125
- w_forget: bfloat16 [2048, 1024], P(None, 'tp'), may hold values from -0.125 to 0.125
- w_input: bfloat16 [2048, 1024], P(None, 'tp'), may hold values from -0.125 to 0.125
- w_outgate: bfloat16 [2048, 1024], P(None, 'tp'), may hold values from -0.125 to 0.125
- w_conv_h: bfloat16 [2048, 1024], P(None, 'tp'), may hold values from -0.125 to 0.125
- w_conv_b: bfloat16 [2048, 1024], P(None, 'tp'), may hold values from -0.125 to 0.125
- w_conv_c: bfloat16 [2048, 1024], P(None, 'tp'), may hold values from -0.125 to 0.125
- forget_floor: float32 [1024], P('tp'), may hold values from 0.84 to 1
- forget_leak: float32 [8192, 1024], P('sp', 'tp'), may hold values from -1 to 0
- state_gain: float32 [128], replicated, may hold values from 0.1 to 1.9
- conv_taps: bfloat16 [3, 1024], P(None, 'tp'), may hold values from -3.5 to 3.5
- group_gain: float32 [128], replicated, may hold values from 0.1 to 1.9
- out_state: bfloat16 [1024, 2048], P('tp'), may hold values from -0.1875 to 0.1875
- out_conv: bfloat16 [1024, 2048], P('tp'), may hold values from -0.1875 to 0.1875
Outputs:
- mixed_out: bfloat16 [8192, 2048], P('sp', 'tp')
The draws below stay inside these ranges and needn't reach their ends.
All inputs are finite; a program needn't handle non-finite values.
Results may differ from the reference program's by a relative error of at most 0.015.
Values may be sent and summed in bfloat16 or wider, within the bound.
A program may use at most 128 MiB of HBM per device.

```python
import jax
import jax.numpy as jnp
from jax import lax

D = 2048
GROUP_FEATURES = 128
MIXER_COUNT = 8
CONV_CH = 1024
BLOCK = 64
TAPS = 3
TOK_DEV = 1024
STEP_COUNT = 8192
STATE_W = 1024
MIX = 2048


def draw_forget_floor(key, part):
    key_fast, key_gap, key_slow = jax.random.split(jax.random.fold_in(key, 11), 3)
    share = 0.5
    is_fast = jax.random.uniform(key_fast, (MIXER_COUNT,)) < share
    is_fast = jnp.repeat(is_fast, GROUP_FEATURES)
    fast_gap = jnp.exp(jax.random.uniform(key_gap, (STATE_W,), jnp.float32, jnp.log(0.05), jnp.log(0.15)))
    slow_gap = jnp.exp(jax.random.uniform(key_slow, (STATE_W,), jnp.float32, jnp.log(0.2), jnp.log(1.0))) / STEP_COUNT
    return (1.0 - jnp.where(is_fast, fast_gap, slow_gap)).astype(jnp.float32)


def draw_forget_leak(key, part):
    key_scale, random_seed_site, key_depth, key_jitter = jax.random.split(jax.random.fold_in(key, 23), 4)
    nblk = STEP_COUNT // TOK_DEV
    low, high = (jnp.log(0.5), jnp.log(2.0))
    block_scale = jnp.exp(jax.random.uniform(key_scale, (nblk, MIXER_COUNT), jnp.float32, low, high))
    block_scale = jnp.repeat(jnp.repeat(block_scale, TOK_DEV, axis=0), GROUP_FEATURES, axis=1)
    jitter = jax.random.uniform(key_jitter, (STEP_COUNT, STATE_W), jnp.float32, 0.5, 1.5)
    starting_shift = -0.2 / STEP_COUNT * block_scale * jitter
    span_start = jax.random.randint(random_seed_site, (3, MIXER_COUNT), 0, STEP_COUNT)
    layer_number = jax.random.uniform(key_depth, (3, MIXER_COUNT), jnp.float32, jnp.log(0.5), jnp.log(0.8))
    element_places = jnp.arange(STEP_COUNT)[:, None]
    span_sizes = jnp.zeros((STEP_COUNT, MIXER_COUNT), jnp.float32)
    for entry_number in range(3):
        span_sizes = span_sizes + jnp.where(element_places == span_start[entry_number][None, :], layer_number[entry_number][None, :], 0.0)
    return (starting_shift + jnp.repeat(span_sizes, GROUP_FEATURES, axis=1)).astype(jnp.float32)


def with_spikes(values, key, source, target, parts, factor):
    owner, partner = [(jnp.arange(values.shape[position]) // (values.shape[position] // parts)).reshape([-1 if axis == position else 1 for axis in range(values.ndim)]) for position in (source, target)]
    chosen = jax.random.permutation(key, parts)[partner]
    strong = (owner == chosen) | (owner == (partner + parts // 2) % parts)
    return jnp.where(strong, factor * values, values)


def levels(key, dims, pieces, least, largest):
    level, own = 1.0, jax.random.fold_in(key, 6)
    for dim, parts in pieces:
        steps = jnp.exp(jax.random.uniform(jax.random.fold_in(own, dim), (parts,), jnp.float32, least / len(pieces), largest / len(pieces)))
        level = level * jnp.repeat(steps, dims[dim] // parts).reshape([-1 if axis == dim else 1 for axis in range(len(dims))])
    return level


def centred(rng, extent, spread, reach, cuts=(), held_as=jnp.bfloat16):
    loudness = levels(rng, extent, cuts, -0.22, 0.18) if cuts else 1.0
    array = jax.random.normal(rng, extent, jnp.float32) * spread * loudness
    return jnp.minimum(jnp.maximum(array, -reach), reach).astype(held_as)


def heavy_noise(own_key, dims, width, limit, shards, heavy, dtype=jnp.bfloat16):
    values = width * jax.random.normal(own_key, dims, jnp.float32)
    if shards:
        values = values * levels(own_key, dims, shards, -0.22, 0.18)
    return jnp.clip(with_spikes(values, jax.random.fold_in(own_key, 3), *heavy), -limit, limit).astype(dtype)


def setup_inputs(seed: int = 0) -> dict:
    streams_of = jax.random.split(jax.random.key(seed), 17)
    return {
        "tokens": centred(streams_of[0], (STEP_COUNT, D), 1.0, 6.0, ((0, 8),)),
        "in_gain": jnp.clip(1.0 + 0.18 * jax.random.normal(streams_of[1], (D,), jnp.float32), 0.1, 1.9),
        "w_query": centred(streams_of[2], (D, STATE_W), D ** -0.5, 0.125, ((1, 4),)),
        "w_forget": centred(streams_of[3], (D, STATE_W), D ** -0.5, 0.125, ((1, 4),)),
        "w_input": centred(streams_of[4], (D, STATE_W), D ** -0.5, 0.125, ((1, 4),)),
        "w_outgate": centred(streams_of[5], (D, STATE_W), D ** -0.5, 0.125, ((1, 4),)),
        "w_conv_h": centred(streams_of[6], (D, CONV_CH), D ** -0.5, 0.125, ((1, 4),)),
        "w_conv_b": centred(streams_of[7], (D, CONV_CH), D ** -0.5, 0.125, ((1, 4),)),
        "w_conv_c": centred(streams_of[8], (D, CONV_CH), D ** -0.5, 0.125, ((1, 4),)),
        "forget_floor": draw_forget_floor(jax.random.fold_in(streams_of[16], 71), 0),
        "forget_leak": draw_forget_leak(jax.random.fold_in(streams_of[16], 71), 0),
        "state_gain": jnp.clip(1.0 + 0.18 * jax.random.normal(streams_of[11], (GROUP_FEATURES,), jnp.float32), 0.1, 1.9),
        "conv_taps": centred(streams_of[12], (TAPS, CONV_CH), TAPS ** -0.5, 3.5, ((1, 4),)),
        "group_gain": jnp.clip(1.0 + 0.18 * jax.random.normal(streams_of[13], (GROUP_FEATURES,), jnp.float32), 0.1, 1.9),
        "out_state": heavy_noise(streams_of[14], (STATE_W, D), MIX ** -0.5, 0.1875, ((0, 4),), (0, 1, 4, 2.0)),
        "out_conv": heavy_noise(streams_of[15], (CONV_CH, D), MIX ** -0.5, 0.1875, ((0, 4),), (0, 1, 4, 2.0)),
    }


norm_eps = 1e-06
highest = lax.Precision.HIGHEST

def rms_rows(values, gain):
    scale = lax.rsqrt(lax.optimization_barrier(jnp.mean(values * values, axis=-1, keepdims=True)) + norm_eps)
    return values * scale * gain.astype(jnp.float32)

def state_block(carry_state, inputs):
    query_blk, key_blk, value_blk, logf_blk = inputs
    cum_log = jnp.cumsum(logf_blk, axis=1)
    carried = jnp.einsum('hcd,hde->hce', query_blk * jnp.exp(cum_log), carry_state, precision=highest)
    length = logf_blk.shape[1]
    causal = (jnp.arange(length)[:, None] >= jnp.arange(length)[None, :])[None, :, :, None]
    diff_log = cum_log[:, :, None, :] - cum_log[:, None, :, :]
    decay_all = jnp.exp(jnp.where(causal, diff_log, -jnp.inf))
    scores = jnp.einsum('hid,hjd,hijd->hij', query_blk, key_blk, decay_all, precision=highest)
    result = carried + jnp.einsum('hij,hje->hie', scores, value_blk, precision=highest)
    last_log = cum_log[:, -1, :]
    fresh = jnp.einsum('hcd,hce->hde', key_blk * jnp.exp(last_log[:, None, :] - cum_log), value_blk, precision=highest)
    new_state = jnp.exp(last_log)[:, :, None] * carry_state + fresh
    return (new_state, result)

def reference(tokens, in_gain, w_query, w_forget, w_input, w_outgate, w_conv_h, w_conv_b, w_conv_c, forget_floor, forget_leak, state_gain, conv_taps, group_gain, out_state, out_conv):
    count = tokens.shape[0]
    heads = MIXER_COUNT
    normed = rms_rows(tokens.astype(jnp.float32), in_gain).astype(jnp.bfloat16)

    def project(weight):
        return jnp.dot(normed, weight, preferred_element_type=jnp.float32).astype(jnp.bfloat16)
    proj_query = project(w_query)
    proj_forget = project(w_forget)
    proj_input = project(w_input)
    proj_outgate = project(w_outgate)
    proj_h = project(w_conv_h)
    proj_b = project(w_conv_b)
    proj_c = project(w_conv_c)
    gate_logit = proj_forget.astype(jnp.float32)
    log_forget = jnp.logaddexp(jnp.log(forget_floor), jnp.log1p(-forget_floor) + jax.nn.log_sigmoid(gate_logit)) + forget_leak
    key_gate = (1.0 - forget_floor) * jax.nn.sigmoid(-gate_logit)
    query_act = jax.nn.silu(proj_query.astype(jnp.float32))
    value_f = proj_input.astype(jnp.float32)
    nblk = count // BLOCK

    def to_blocks(arr):
        return arr.reshape(nblk, BLOCK, heads, GROUP_FEATURES).transpose(0, 2, 1, 3)
    start_state = jnp.zeros((heads, GROUP_FEATURES, GROUP_FEATURES), jnp.float32)
    _, outputs = lax.scan(state_block, start_state, (to_blocks(query_act), to_blocks(key_gate), to_blocks(value_f), to_blocks(log_forget)))
    state_read = outputs.transpose(0, 2, 1, 3).reshape(count, heads, GROUP_FEATURES)
    out_gate = jax.nn.silu(proj_outgate.astype(jnp.float32)).reshape(count, heads, GROUP_FEATURES)
    state_res = (rms_rows(state_read, state_gain) * out_gate).reshape(count, STATE_W).astype(jnp.bfloat16)
    conv_in = (proj_c.astype(jnp.float32) * proj_h.astype(jnp.float32)).astype(jnp.bfloat16)
    padded = jnp.concatenate([jnp.zeros((TAPS - 1, CONV_CH), jnp.bfloat16), conv_in], axis=0).astype(jnp.float32)
    taps_f = conv_taps.astype(jnp.float32)
    conv_sum = jnp.zeros((count, CONV_CH), jnp.float32)
    for offset in range(TAPS):
        conv_sum = conv_sum + taps_f[offset][None, :] * padded[offset:offset + count]
    gated = (proj_b.astype(jnp.float32) * conv_sum).reshape(count, CONV_CH // GROUP_FEATURES, GROUP_FEATURES)
    conv_res = rms_rows(gated, group_gain).reshape(count, CONV_CH).astype(jnp.bfloat16)
    total = jnp.dot(state_res, out_state, preferred_element_type=jnp.float32)
    total = total + jnp.dot(conv_res, out_conv, preferred_element_type=jnp.float32)
    return total.astype(jnp.bfloat16)
```

```python
import functools

import jax
import jax.numpy as jnp
from jax import lax
from jax.experimental import pallas as pl
from jax.experimental.pallas import tpu as pltpu
from jax.sharding import PartitionSpec as P

GROUP_FEATURES = 128
CHUNK = 128
ROWS = 256
TAPS = 3
HALO = 8
HEAD = 16
SHARE = 4
CONV, MIX = 0, 1

norm_eps = 1e-06
f32 = jnp.float32
bf16 = jnp.bfloat16


def dot(a, b, dims=((1,), (0,))):
    return lax.dot_general(a, b, (dims, ((), ())), preferred_element_type=f32)


def rms(values):
    return values * lax.rsqrt(jnp.mean(values * values, axis=-1, keepdims=True) + norm_eps)


def per_group(values, gain):
    parts = []
    for g in range(values.shape[1] // GROUP_FEATURES):
        parts.append(rms(values[:, g * GROUP_FEATURES : (g + 1) * GROUP_FEATURES]) * gain)
    return jnp.concatenate(parts, axis=1)


def head_slice(h):
    return slice(h * GROUP_FEATURES, (h + 1) * GROUP_FEATURES)


def prefix_sum(ones, values):
    high = values.astype(bf16)
    rest = values - high.astype(f32)
    middle = rest.astype(bf16)
    low = (rest - middle.astype(f32)).astype(bf16)
    return dot(ones, jnp.concatenate([high, middle, low], axis=0))


def fused_kernel(
    tp, sp, share,
    tokens, in_gain, wq, wf, wi, wg, wh, wb, wc, floor, leak, state_gain, taps, group_gain,
    out_state, out_conv, result,
    normed_all, w_scan, w_conv, w_read, cums, key_mid, value_all, olds, offsets,
    pad, state, offset, read, qdev, gate, conv_all, mix_all, columns, acc_all,
    sent_state, peer_state, peer_log, sent_total, sent_log, totals, total_logs,
    rim, tail, head_conv, head_gate, incoming,
    tok_sem, leak_sem, w_sem, own_sem,
    pair_send, pair_recv, piece_send, piece_recv, mate_send,
    blk_send, fwd_send, blk_recv, l1_send, l1_recv, l2_send, l2_recv, rim_send, rim_recv,
):
    me, place = lax.axis_index("tp"), lax.axis_index("sp")
    partner = me + 1 - 2 * lax.rem(me, 2)
    chips = tp // 2
    chip = lax.div(me, 2)
    core = lax.rem(me, 2)
    count, feats = normed_all.shape
    width = value_all.shape[1]
    channels = pad.shape[1]
    rows = ROWS
    nb = count // rows
    ncols = result.shape[1]
    heads = state.shape[0]
    piece = width // share
    mine = lax.rem(place, share)
    base = place - mine
    twin = place + 1 - 2 * lax.rem(place, 2)
    member = lax.rem(place, 2)
    pair = lax.div(place, 2)
    held = (conv_all, mix_all)
    outs = (out_conv, out_state)

    def block(t):
        return pl.ds(pl.multiple_of(t * rows, rows), rows)

    def token_copy(t):
        return pltpu.make_async_copy(tokens.at[block(t)], normed_all.at[block(t)], tok_sem.at[t])

    leak_copy = pltpu.make_async_copy(leak, cums, leak_sem.at[0])
    weights = ((wf, w_scan, 0), (wi, w_scan, 1), (wc, w_conv, 0), (wh, w_conv, 1),
               (wb, w_conv, 2), (wq, w_read, 0), (wg, w_read, 1))

    def weight_copy(n):
        src, dst, slot = weights[n]
        return pltpu.make_async_copy(
            src, dst.at[:, slot * width : (slot + 1) * width], w_sem.at[n]
        )

    def cols_of(device):
        return pl.ds(pl.multiple_of(device * ncols, ncols), ncols)

    def piece_rows(g):
        return pl.ds(pl.multiple_of(g * piece, piece), piece)

    def own_columns(kind):
        return pltpu.make_async_copy(
            outs[kind].at[:, cols_of(me)], columns.at[kind, me], own_sem.at[kind]
        )

    def pair_columns(kind, origin):
        return pltpu.make_async_remote_copy(
            outs[kind].at[:, cols_of(partner)], columns.at[kind, origin],
            pair_send.at[kind], pair_recv.at[kind], device_id={"tp": partner},
        )

    def far(k, c):
        return lax.rem(chip + k, chips) * 2 + c

    def piece_out(kind, k, c):
        target = far(k, c)
        return pltpu.make_async_remote_copy(
            outs[kind].at[piece_rows(mine), cols_of(target)],
            columns.at[kind, me, piece_rows(mine)],
            piece_send.at[kind, k, c], piece_recv.at[kind, me, mine], device_id={"tp": target},
        )

    def piece_in(kind, origin, g):
        ref = columns.at[kind, origin, piece_rows(g)]
        return pltpu.make_async_remote_copy(
            ref, ref, mate_send.at[kind, 0, 0, 0], piece_recv.at[kind, origin, g],
            device_id={"tp": partner},
        )

    def mate_copy(kind, k, c, r):
        ref = columns.at[kind, far(k, c), piece_rows(mine)]
        return pltpu.make_async_remote_copy(
            ref, ref, mate_send.at[kind, k, c, r], piece_recv.at[kind, far(k, c), mine],
            device_id={"sp": base + lax.rem(mine + r, share)},
        )

    far_devices = [(k, c) for k in range(1, chips) for c in range(2)]

    def span(kind, t):
        if kind == CONV and isinstance(t, int):
            if t == 0:
                return pl.ds(HEAD, rows - HEAD)
            if t == nb:
                return pl.ds(0, HEAD)
        return block(t)

    def block_copy(kind, t, origin, target, send):
        ref = held[kind].at[origin, span(kind, t)]
        return pltpu.make_async_remote_copy(
            ref, ref, send, blk_recv.at[kind, origin, t], device_id={"tp": target}
        )

    def own_copies(kind, t):
        out = []
        for k in range(1, chips):
            out.append(block_copy(kind, t, me, far(k, core), blk_send.at[kind, k, t]))
        out.append(block_copy(kind, t, me, partner, blk_send.at[kind, 0, t]))
        return out

    def relays(kind, t):
        return [
            block_copy(kind, t, far(k, core), partner, fwd_send.at[kind, k, t])
            for k in range(1, chips)
        ]

    def start(copies):
        for copy in copies:
            copy.start()

    def relay(kind, t):
        for copy in relays(kind, t):
            copy.wait_recv()
            copy.start()

    def arrived(kind, t, origin):
        block_copy(kind, t, origin, partner, blk_send.at[kind, 0, t]).wait_recv()

    def twin_copies():
        to = {"sp": twin}
        return (
            pltpu.make_async_remote_copy(
                sent_state, peer_state, l1_send.at[0], l1_recv.at[0], device_id=to
            ),
            pltpu.make_async_remote_copy(
                offset, peer_log, l1_send.at[1], l1_recv.at[1], device_id=to
            ),
        )

    def total_copies(k, source):
        to = {"sp": lax.rem(place + 2 * k, sp)}
        return (
            pltpu.make_async_remote_copy(
                sent_total, totals.at[source], l2_send.at[0, k], l2_recv.at[0, source],
                device_id=to,
            ),
            pltpu.make_async_remote_copy(
                sent_log, total_logs.at[source], l2_send.at[1, k], l2_recv.at[1, source],
                device_id=to,
            ),
        )

    rim_copy = pltpu.make_async_remote_copy(
        tail, rim, rim_send.at[0], rim_recv.at[0], device_id={"sp": lax.rem(place + 1, sp)}
    )

    token_copy(0).start()
    weight_copy(0).start()
    weight_copy(1).start()
    leak_copy.start()
    for t in range(1, nb):
        token_copy(t).start()
    for n in range(2, 7):
        weight_copy(n).start()
    barrier = pltpu.get_barrier_semaphore()
    for k in range(1, tp):
        pl.semaphore_signal(barrier, inc=1, device_id={"tp": lax.rem(me + k, tp)})
    for k in range(1, sp):
        pl.semaphore_signal(barrier, inc=1, device_id={"sp": lax.rem(place + k, sp)})
    pl.semaphore_wait(barrier, tp + sp - 2)
    for kind in (CONV, MIX):
        for k, c in far_devices:
            piece_out(kind, k, c).start()
    for kind in (CONV, MIX):
        pair_columns(kind, me).start()
        own_columns(kind).start()

    state[...] = jnp.zeros_like(state)
    offset[...] = jnp.zeros_like(offset)
    pad[0:HALO, :] = jnp.zeros((HALO, channels), f32)

    r = lax.broadcasted_iota(jnp.int32, (CHUNK, CHUNK), 0)
    c = lax.broadcasted_iota(jnp.int32, (CHUNK, CHUNK), 1)
    causal = r >= c
    ones = jnp.concatenate([causal.astype(f32)] * 3, axis=1).astype(bf16)
    w_taps = taps[...].astype(f32)

    weight_copy(0).wait()
    weight_copy(1).wait()
    leak_copy.wait()

    def scan_block(t, _):
        token_copy(t).wait()
        at = block(t)
        normed = (rms(normed_all[at, :].astype(f32)) * in_gain[...]).astype(bf16)
        normed_all[at, :] = normed
        both = dot(normed, w_scan[...])
        x = both[:, :width].astype(bf16).astype(f32)
        value = both[:, width:].astype(bf16)
        value_all[at, :] = value
        key = (1.0 - floor[...]) * jax.nn.sigmoid(-x)
        logf = jnp.log(1.0 - key) + cums[at, :]
        for b in range(rows // CHUNK):
            lo, hi = b * CHUNK, (b + 1) * CHUNK
            where = pl.ds(pl.multiple_of(t * rows + lo, CHUNK), CHUNK)
            number = t * (rows // CHUNK) + b
            cum = prefix_sum(ones, logf[lo:hi])
            mid = cum[CHUNK // 2 - 1 : CHUNK // 2]
            last = cum[CHUNK - 1 : CHUNK]
            k_mid = key[lo:hi] * jnp.exp(mid - cum)
            k_end = (k_mid * jnp.exp(last - mid)).astype(bf16)
            cums[where, :] = cum
            key_mid[where, :] = k_mid.astype(bf16)
            offsets[number] = offset[...]
            for h in range(heads):
                s = head_slice(h)
                old = state[h]
                olds[number, h] = old.astype(bf16)
                state[h] = old * jnp.exp(last[:, s]) + dot(
                    value[lo:hi, s], k_end[:, s], ((0,), (0,))
                )
            offset[...] += last
        return 0

    lax.fori_loop(0, nb, scan_block, 0)
    sent_state[...] = state[...].astype(bf16)
    start(twin_copies())

    for n in (2, 3, 4):
        weight_copy(n).wait()

    def conv_block(t, _):
        at = block(t)
        three = dot(normed_all[at, :], w_conv[...])
        first = three[:, :channels].astype(bf16).astype(f32)
        second = three[:, channels : 2 * channels].astype(bf16).astype(f32)
        proj_b = three[:, 2 * channels :].astype(bf16).astype(f32)
        conv_in = (first * second).astype(bf16).astype(f32)
        pad[HALO : HALO + rows, :] = conv_in
        total = w_taps[TAPS - 1 : TAPS] * conv_in
        for j in range(TAPS - 1):
            lo = HALO - (TAPS - 1) + j
            total += w_taps[j : j + 1] * pad[lo : lo + rows, :]
        conv_all[me, at, :] = per_group(proj_b * total, group_gain[...]).astype(bf16)

        @pl.when(t == 0)
        def _():
            head_conv[...] = conv_in[:HALO]
            head_gate[...] = proj_b[:HALO]
            start(own_copies(CONV, 0))

        @pl.when(t > 0)
        def _():
            start(own_copies(CONV, t))

        pad[0:HALO, :] = conv_in[rows - HALO :]

        @pl.when(t == nb - 1)
        def _():
            tail[...] = conv_in[rows - HALO :]
            rim_copy.start()

        @pl.when(t == min(2, nb - 1))
        def _():
            for copy in twin_copies():
                copy.wait_recv()
            log_second = jnp.where(member == 0, peer_log[0:1, :], offset[0:1, :])
            decay = jnp.exp(log_second)
            for h in range(heads):
                own, other = state[h], peer_state[h].astype(f32)
                early = jnp.where(member == 0, own, other)
                late = jnp.where(member == 0, other, own)
                sent_total[h] = (early * decay[:, head_slice(h)] + late).astype(bf16)
            sent_log[...] = offset[...] + peer_log[...]
            for k in range(1, sp // 2):
                @pl.when(pair + k < sp // 2)
                def _():
                    start(total_copies(k, pair))

        return 0

    lax.fori_loop(0, nb, conv_block, 0)

    for n in (5, 6):
        weight_copy(n).wait()

    def read_block(t, _):
        at = block(t)
        both = dot(normed_all[at, :], w_read[...])
        query = jax.nn.silu(both[:, :width].astype(bf16).astype(f32))
        outgate = jax.nn.silu(both[:, width:].astype(bf16).astype(f32))
        for h in range(heads):
            s = head_slice(h)
            gate[at, s] = outgate[:, s] * state_gain[...]
        for b in range(rows // CHUNK):
            lo, hi = b * CHUNK, (b + 1) * CHUNK
            where = pl.ds(pl.multiple_of(t * rows + lo, CHUNK), CHUNK)
            number = t * (rows // CHUNK) + b
            cum = cums[where, :]
            mid = cum[CHUNK // 2 - 1 : CHUNK // 2]
            q_mid = query[lo:hi] * jnp.exp(cum - mid)
            q_all = q_mid * jnp.exp(mid)
            qdev[where, :] = (q_all * jnp.exp(offsets[number, 0:1, :])).astype(bf16)
            q_mid, q_all = q_mid.astype(bf16), q_all.astype(bf16)
            for h in range(heads):
                s = head_slice(h)
                scores = dot(q_mid[:, s], key_mid[where, s], ((1,), (1,)))
                scores = jnp.where(causal, scores, 0.0).astype(bf16)
                read[where, s] = dot(scores, value_all[where, s]) + dot(
                    q_all[:, s], olds[number, h], ((1,), (1,))
                )

        @pl.when(t == 0)
        def _():
            rim_copy.wait_recv()
            before = jnp.where(place > 0, rim[...], 0.0)
            ext = jnp.concatenate([before, head_conv[...]], axis=0)
            fixed = w_taps[TAPS - 1 : TAPS] * head_conv[...]
            for j in range(TAPS - 1):
                lo = HALO - (TAPS - 1) + j
                fixed += w_taps[j : j + 1] * ext[lo : lo + HALO]
            fixed = per_group(head_gate[...] * fixed, group_gain[...])
            conv_all[me, 0:HALO, :] = fixed.astype(bf16)
            start(own_copies(CONV, nb))

        return 0

    lax.fori_loop(0, nb, read_block, 0)

    for kind in (CONV, MIX):
        for k, c in far_devices:
            piece_in(kind, far(k, c), mine).wait_recv()
            for n in range(1, share):
                mate_copy(kind, k, c, n).start()
    for kind in (CONV, MIX):
        own_columns(kind).wait()
        pair_columns(kind, partner).wait_recv()

    def near(kind, t):
        out = dot(held[kind][me, block(t), :], columns[kind, me])
        return out + dot(held[kind][partner, block(t), :], columns[kind, partner])

    def near_conv(t, _):
        acc_all[block(t), :] = near(CONV, t)
        return 0

    arrived(CONV, 0, partner)
    arrived(CONV, nb, partner)

    def conv_partner(t, _):
        arrived(CONV, t + 1, partner)
        return 0

    lax.fori_loop(0, nb - 1, conv_partner, 0)
    lax.fori_loop(0, nb, near_conv, 0)

    for k in range(1, sp // 2):
        @pl.when(pair >= k)
        def _():
            for copy in total_copies(k, pair - k):
                copy.wait_recv()
    incoming[...] = jnp.zeros_like(incoming)

    def hop(p, _):
        decay = jnp.exp(total_logs[p, 0:1, :])
        for h in range(heads):
            incoming[h] = incoming[h] * decay[:, head_slice(h)] + totals[p, h].astype(f32)
        return 0

    lax.fori_loop(0, pair, hop, 0)
    decay = jnp.exp(peer_log[0:1, :])
    for h in range(heads):
        through = incoming[h] * decay[:, head_slice(h)] + peer_state[h].astype(f32)
        incoming[h] = jnp.where(member == 0, incoming[h], through)

    def merge(t, _):
        at = block(t)
        for h in range(heads):
            s = head_slice(h)
            whole = read[at, s] + dot(qdev[at, s], incoming[h].astype(bf16), ((1,), (1,)))
            mix_all[me, at, s] = (rms(whole) * gate[at, s]).astype(bf16)
        start(own_copies(MIX, t))
        return 0

    lax.fori_loop(0, nb, merge, 0)

    def near_mix(t, _):
        arrived(MIX, t, partner)
        acc_all[block(t), :] += near(MIX, t)
        return 0

    lax.fori_loop(0, nb, near_mix, 0)

    def conv_relay(t, _):
        relay(CONV, t + 1)
        return 0

    relay(CONV, 0)
    lax.fori_loop(0, nb - 1, conv_relay, 0)
    relay(CONV, nb)
    for kind in (CONV, MIX):
        for k, c in far_devices:
            for n in range(1, share):
                piece_in(kind, far(k, c), lax.rem(mine + n, share)).wait_recv()
    for k in range(1, chips):
        arrived(CONV, 0, far(k, 1 - core))
        arrived(CONV, nb, far(k, 1 - core))

    def conv_arrivals(t, _):
        for k in range(1, chips):
            arrived(CONV, t + 1, far(k, 1 - core))
        return 0

    lax.fori_loop(0, nb - 1, conv_arrivals, 0)

    def far_conv(t, _):
        acc = acc_all[block(t), :]
        for k, c in far_devices:
            origin = far(k, c)
            acc += dot(conv_all[origin, block(t), :], columns[CONV, origin])
        acc_all[block(t), :] = acc
        return 0

    lax.fori_loop(0, nb, far_conv, 0)

    def finish(t, _):
        relay(MIX, t)
        for k in range(1, chips):
            arrived(MIX, t, far(k, 1 - core))
        acc = acc_all[block(t), :]
        for k, c in far_devices:
            origin = far(k, c)
            acc += dot(mix_all[origin, block(t), :], columns[MIX, origin])
        result[block(t), :] = acc.astype(bf16)
        return 0

    lax.fori_loop(0, nb, finish, 0)

    def drain(t, _):
        for copy in own_copies(MIX, t) + relays(MIX, t):
            copy.wait_send()
        return 0

    def drain_conv(t, _):
        for copy in own_copies(CONV, t + 1) + relays(CONV, t + 1):
            copy.wait_send()
        return 0

    lax.fori_loop(0, nb, drain, 0)
    lax.fori_loop(0, nb - 1, drain_conv, 0)
    for t in (0, nb):
        for copy in own_copies(CONV, t) + relays(CONV, t):
            copy.wait_send()
    for kind in (CONV, MIX):
        pair_columns(kind, me).wait_send()
        for k, c in far_devices:
            piece_out(kind, k, c).wait_send()
            for n in range(1, share):
                mate_copy(kind, k, c, n).wait_send()
    rim_copy.wait_send()
    for copy in twin_copies():
        copy.wait_send()
    for k in range(1, sp // 2):
        @pl.when(pair + k < sp // 2)
        def _():
            for copy in total_copies(k, pair):
                copy.wait_send()


def body(
    tokens, in_gain, w_query, w_forget, w_input, w_outgate, w_conv_h, w_conv_b, w_conv_c,
    forget_floor, forget_leak, state_gain, conv_taps, group_gain, out_state, out_conv,
):
    count, feats = tokens.shape
    width, channels = w_query.shape[1], w_conv_h.shape[1]
    heads = width // GROUP_FEATURES
    tp, sp = lax.axis_size("tp"), lax.axis_size("sp")
    ncols, nb, chips = out_state.shape[1] // tp, count // ROWS, tp // 2
    share = min(SHARE, sp)
    chunks, pairs = count // CHUNK, sp // 2

    hbm = pl.BlockSpec(memory_space=pl.ANY)
    vmem = pl.BlockSpec(memory_space=pltpu.VMEM)
    sems = pltpu.SemaphoreType.DMA
    square = (heads, GROUP_FEATURES, GROUP_FEATURES)
    return pl.pallas_call(
        functools.partial(fused_kernel, tp, sp, share),
        in_specs=[hbm, vmem] + [hbm] * 7 + [vmem, hbm, vmem, vmem, vmem, hbm, hbm],
        out_specs=vmem,
        out_shape=jax.ShapeDtypeStruct((count, ncols), bf16),
        scratch_shapes=[
            pltpu.VMEM((count, feats), bf16),
            pltpu.VMEM((feats, 2 * width), bf16),
            pltpu.VMEM((feats, 3 * channels), bf16),
            pltpu.VMEM((feats, 2 * width), bf16),
            pltpu.VMEM((count, width), f32),
            pltpu.VMEM((count, width), bf16),
            pltpu.VMEM((count, width), bf16),
            pltpu.VMEM((chunks,) + square, bf16),
            pltpu.VMEM((chunks, HALO, width), f32),
            pltpu.VMEM((HALO + ROWS, channels), f32),
            pltpu.VMEM(square, f32),
            pltpu.VMEM((HALO, width), f32),
            pltpu.VMEM((count, width), f32),
            pltpu.VMEM((count, width), bf16),
            pltpu.VMEM((count, width), f32),
            pltpu.VMEM((tp, count, channels), bf16),
            pltpu.VMEM((tp, count, width), bf16),
            pltpu.VMEM((2, tp, width, ncols), bf16),
            pltpu.VMEM((count, ncols), f32),
            pltpu.VMEM(square, bf16),
            pltpu.VMEM(square, bf16),
            pltpu.VMEM((HALO, width), f32),
            pltpu.VMEM(square, bf16),
            pltpu.VMEM((HALO, width), f32),
            pltpu.VMEM((pairs,) + square, bf16),
            pltpu.VMEM((pairs, HALO, width), f32),
            pltpu.VMEM((HALO, channels), f32),
            pltpu.VMEM((HALO, channels), f32),
            pltpu.VMEM((HALO, channels), f32),
            pltpu.VMEM((HALO, channels), f32),
            pltpu.VMEM(square, f32),
            sems((nb,)), sems((1,)), sems((7,)), sems((2,)),
            sems((2,)), sems((2,)), sems((2, chips, 2)), sems((2, tp, share)),
            sems((2, chips, 2, share)),
            sems((2, chips, nb + 1)), sems((2, chips, nb + 1)), sems((2, tp, nb + 1)),
            sems((2,)), sems((2,)), sems((2, pairs)), sems((2, pairs)), sems((1,)), sems((1,)),
        ],
        compiler_params=pltpu.CompilerParams(
            vmem_limit_bytes=56 * 2**20, collective_id=0, has_side_effects=True
        ),
    )(
        tokens, in_gain[None], w_query, w_forget, w_input, w_outgate, w_conv_h, w_conv_b, w_conv_c,
        forget_floor[None], forget_leak, state_gain[None], conv_taps, group_gain[None],
        out_state, out_conv,
    )


def solution(mesh):
    cols, rows = P(None, "tp"), P("tp", None)
    in_specs = (
        P("sp", None), P(), cols, cols, cols, cols, cols, cols, cols,
        P("tp"), P("sp", "tp"), P(), cols, P(), rows, rows,
    )
    return jax.shard_map(
        body, mesh=mesh, in_specs=in_specs, out_specs=P("sp", "tp"), check_vma=False
    )
```

```python
import functools

import jax
import jax.numpy as jnp
from jax import lax
from jax.experimental import pallas as pl
from jax.experimental.pallas import tpu as pltpu
from jax.sharding import PartitionSpec as P

GROUP_FEATURES = 128
CHUNK = 128
ROWS = 256
TAPS = 3
HALO = 8
HEAD = 16
SHARE = 4
CONV, MIX = 0, 1

norm_eps = 1e-06
f32 = jnp.float32
bf16 = jnp.bfloat16


def dot(a, b, dims=((1,), (0,))):
    return lax.dot_general(a, b, (dims, ((), ())), preferred_element_type=f32)


def rms(values):
    return values * lax.rsqrt(jnp.mean(values * values, axis=-1, keepdims=True) + norm_eps)


def per_group(values, gain):
    parts = []
    for g in range(values.shape[1] // GROUP_FEATURES):
        parts.append(rms(values[:, g * GROUP_FEATURES : (g + 1) * GROUP_FEATURES]) * gain)
    return jnp.concatenate(parts, axis=1)


def head_slice(h):
    return slice(h * GROUP_FEATURES, (h + 1) * GROUP_FEATURES)


def prefix_sum(ones, values):
    high = values.astype(bf16)
    rest = values - high.astype(f32)
    middle = rest.astype(bf16)
    low = (rest - middle.astype(f32)).astype(bf16)
    return dot(ones, jnp.concatenate([high, middle, low], axis=0))


def fused_kernel(
    tp, sp, share,
    tokens, in_gain, wq, wf, wi, wg, wh, wb, wc, floor, leak, state_gain, taps, group_gain,
    out_state, out_conv, result,
    normed_all, w_scan, w_conv, w_read, cums, key_mid, value_all, olds, offsets,
    pad, state, offset, read, qdev, gate, conv_all, mix_all, columns, acc_all,
    sent_state, peer_state, peer_log, sent_total, sent_log, totals, total_logs,
    rim, tail, head_conv, head_gate, incoming,
    tok_sem, leak_sem, w_sem, own_sem,
    pair_send, pair_recv, piece_send, piece_recv, mate_send,
    blk_send, fwd_send, blk_recv, l1_send, l1_recv, l2_send, l2_recv, rim_send, rim_recv, ready, rim_ready,
):
    me, place = lax.axis_index("tp"), lax.axis_index("sp")
    partner = me + 1 - 2 * lax.rem(me, 2)
    chips = tp // 2
    chip = lax.div(me, 2)
    core = lax.rem(me, 2)
    count, feats = normed_all.shape
    width = value_all.shape[1]
    channels = pad.shape[1]
    rows = ROWS
    nb = count // rows
    ncols = result.shape[1]
    heads = state.shape[0]
    piece = width // share
    mine = lax.rem(place, share)
    twin = place + 1 - 2 * lax.rem(place, 2)
    across = share // 2
    step = across - share * lax.div(mine, across)
    mate, mates_piece = place + step, mine + step
    member = lax.rem(place, 2)
    pair = lax.div(place, 2)
    pairs = sp // 2
    before, after = lax.rem(place + sp - 1, sp), lax.rem(place + 1, sp)
    held = (conv_all, mix_all)
    outs = (out_conv, out_state)

    def block(t):
        return pl.ds(pl.multiple_of(t * rows, rows), rows)

    def token_copy(t):
        return pltpu.make_async_copy(tokens.at[block(t)], normed_all.at[block(t)], tok_sem.at[t])

    def leak_copy(t):
        return pltpu.make_async_copy(leak.at[block(t)], cums.at[block(t)], leak_sem.at[t])

    weights = ((wf, w_scan, 0), (wi, w_scan, 1), (wc, w_conv, 0), (wh, w_conv, 1),
               (wb, w_conv, 2), (wq, w_read, 0), (wg, w_read, 1))

    def weight_copy(n):
        src, dst, slot = weights[n]
        return pltpu.make_async_copy(
            src, dst.at[:, slot * width : (slot + 1) * width], w_sem.at[n]
        )

    def cols_of(device):
        return pl.ds(pl.multiple_of(device * ncols, ncols), ncols)

    def piece_rows(g):
        return pl.ds(pl.multiple_of(g * piece, piece), piece)

    def own_columns(kind):
        return pltpu.make_async_copy(
            outs[kind].at[:, cols_of(me)], columns.at[kind, me], own_sem.at[kind]
        )

    def pair_columns(kind, origin):
        return pltpu.make_async_remote_copy(
            outs[kind].at[:, cols_of(partner)], columns.at[kind, origin],
            pair_send.at[kind], pair_recv.at[kind], device_id={"tp": partner},
        )

    def far(k, c):
        return lax.rem(chip + k, chips) * 2 + c

    def piece_out(kind, k, c):
        target = far(k, c)
        return pltpu.make_async_remote_copy(
            outs[kind].at[piece_rows(mine), cols_of(target)],
            columns.at[kind, me, piece_rows(mine)],
            piece_send.at[kind, k, c], piece_recv.at[kind, me, mine], device_id={"tp": target},
        )

    def piece_in(kind, origin, g):
        ref = columns.at[kind, origin, piece_rows(g)]
        return pltpu.make_async_remote_copy(
            ref, ref, mate_send.at[kind, 0, 0, 0], piece_recv.at[kind, origin, g],
            device_id={"tp": partner},
        )

    def pass_on(kind, k, c, n):
        g, to = ((mine, mate), (mine, twin), (mates_piece, twin))[n]
        ref = columns.at[kind, far(k, c), piece_rows(g)]
        return pltpu.make_async_remote_copy(
            ref, ref, mate_send.at[kind, k, c, n], piece_recv.at[kind, far(k, c), g],
            device_id={"sp": to},
        )

    def pass_own(kind):
        for k, c in far_devices:
            piece_in(kind, far(k, c), mine).wait_recv()
            pass_on(kind, k, c, 0).start()
            pass_on(kind, k, c, 1).start()

    def pass_mates(kind):
        for k, c in far_devices:
            piece_in(kind, far(k, c), mates_piece).wait_recv()
            pass_on(kind, k, c, 2).start()

    far_devices = [(k, c) for k in range(1, chips) for c in range(2)]

    def span(kind, t):
        if kind == CONV and isinstance(t, int):
            if t == 0:
                return pl.ds(HEAD, rows - HEAD)
            if t == nb:
                return pl.ds(0, HEAD)
        return block(t)

    def block_copy(kind, t, origin, target, send):
        ref = held[kind].at[origin, span(kind, t)]
        return pltpu.make_async_remote_copy(
            ref, ref, send, blk_recv.at[kind, origin, t], device_id={"tp": target}
        )

    def own_copies(kind, t):
        out = []
        for k in range(1, chips):
            out.append(block_copy(kind, t, me, far(k, core), blk_send.at[kind, k, t]))
        out.append(block_copy(kind, t, me, partner, blk_send.at[kind, 0, t]))
        return out

    def relays(kind, t):
        return [
            block_copy(kind, t, far(k, core), partner, fwd_send.at[kind, k, t])
            for k in range(1, chips)
        ]

    def start(copies):
        for copy in copies:
            copy.start()

    def relay(kind, t):
        for copy in relays(kind, t):
            copy.wait_recv()
            copy.start()

    def arrived(kind, t, origin):
        block_copy(kind, t, origin, partner, blk_send.at[kind, 0, t]).wait_recv()

    def twin_copies():
        to = {"sp": twin}
        return (
            pltpu.make_async_remote_copy(
                sent_state, peer_state, l1_send.at[0], l1_recv.at[0], device_id=to
            ),
            pltpu.make_async_remote_copy(
                offset.at[0:1], peer_log.at[0:1], l1_send.at[1], l1_recv.at[1], device_id=to
            ),
        )

    def total_copies(k, source):
        to = {"sp": lax.rem(place + 2 * k, sp)}
        return (
            pltpu.make_async_remote_copy(
                sent_total, totals.at[source], l2_send.at[0, k], l2_recv.at[0, source],
                device_id=to,
            ),
            pltpu.make_async_remote_copy(
                sent_log.at[0:1], total_logs.at[source, 0:1], l2_send.at[1, k], l2_recv.at[1, source],
                device_id=to,
            ),
        )

    rim_copy = pltpu.make_async_remote_copy(
        tail, rim, rim_send.at[0], rim_recv.at[0], device_id={"sp": after}
    )

    token_copy(0).start()
    weight_copy(0).start()
    weight_copy(1).start()
    leak_copy(0).start()
    barrier = pltpu.get_barrier_semaphore()
    for k in range(1, tp):
        pl.semaphore_signal(barrier, inc=1, device_id={"tp": lax.rem(me + k, tp)})
    for to in (twin, mate):
        pl.semaphore_signal(barrier, inc=1, device_id={"sp": to})
    for k in range(1, pairs):
        @pl.when(pair + k < pairs)
        def _():
            pl.semaphore_signal(barrier, inc=1, device_id={"sp": lax.rem(place + 2 * k, sp)})
    follows = jnp.logical_and(member == 0, pair > 0)
    leads = jnp.logical_and(member == 1, pair < pairs - 1)

    @pl.when(leads)
    def _():
        pl.semaphore_signal(barrier, inc=1, device_id={"sp": after})

    pl.semaphore_wait(barrier, tp + 1 + pair + jnp.where(follows, 1, 0))
    for k in range(1, pairs):
        @pl.when(pair >= k)
        def _():
            pl.semaphore_signal(ready, inc=1, device_id={"sp": lax.rem(place + sp - 2 * k, sp)})

    @pl.when(follows)
    def _():
        pl.semaphore_signal(rim_ready, inc=1, device_id={"sp": before})
    for kind in (CONV, MIX):
        for k, c in far_devices:
            piece_out(kind, k, c).start()
    for kind in (CONV, MIX):
        pair_columns(kind, me).start()
        own_columns(kind).start()

    state[...] = jnp.zeros_like(state)
    offset[...] = jnp.zeros_like(offset)
    pad[0:HALO, :] = jnp.zeros((HALO, channels), f32)

    r = lax.broadcasted_iota(jnp.int32, (CHUNK, CHUNK), 0)
    c = lax.broadcasted_iota(jnp.int32, (CHUNK, CHUNK), 1)
    causal = r >= c
    ones = jnp.concatenate([causal.astype(f32)] * 3, axis=1).astype(bf16)
    w_taps = taps[...].astype(f32)

    weight_copy(0).wait()
    weight_copy(1).wait()
    for t in range(1, nb):
        token_copy(t).start()
        leak_copy(t).start()
    for n in range(2, 7):
        weight_copy(n).start()

    def scan_block(t, _):
        token_copy(t).wait()
        leak_copy(t).wait()
        at = block(t)
        normed = (rms(normed_all[at, :].astype(f32)) * in_gain[...]).astype(bf16)
        normed_all[at, :] = normed
        both = dot(normed, w_scan[...])
        x = both[:, :width].astype(bf16).astype(f32)
        value = both[:, width:].astype(bf16)
        value_all[at, :] = value
        key = (1.0 - floor[...]) * jax.nn.sigmoid(-x)
        logf = jnp.log(1.0 - key) + cums[at, :]
        for b in range(rows // CHUNK):
            lo, hi = b * CHUNK, (b + 1) * CHUNK
            where = pl.ds(pl.multiple_of(t * rows + lo, CHUNK), CHUNK)
            number = t * (rows // CHUNK) + b
            cum = prefix_sum(ones, logf[lo:hi])
            mid = cum[CHUNK // 2 - 1 : CHUNK // 2]
            last = cum[CHUNK - 1 : CHUNK]
            k_mid = key[lo:hi] * jnp.exp(mid - cum)
            k_end = (k_mid * jnp.exp(last - mid)).astype(bf16)
            cums[where, :] = cum
            key_mid[where, :] = k_mid.astype(bf16)
            offsets[number] = offset[...]
            for h in range(heads):
                s = head_slice(h)
                old = state[h]
                olds[number, h] = old.astype(bf16)
                state[h] = old * jnp.exp(last[:, s]) + dot(
                    value[lo:hi, s], k_end[:, s], ((0,), (0,))
                )
            offset[...] += last
        return 0

    lax.fori_loop(0, nb, scan_block, 0)
    sent_state[...] = state[...].astype(bf16)
    start(twin_copies())
    pass_own(CONV)
    pass_own(MIX)

    for n in (2, 3, 4):
        weight_copy(n).wait()

    def conv_block(t, _):
        at = block(t)
        three = dot(normed_all[at, :], w_conv[...])
        first = three[:, :channels].astype(bf16).astype(f32)
        second = three[:, channels : 2 * channels].astype(bf16).astype(f32)
        proj_b = three[:, 2 * channels :].astype(bf16).astype(f32)
        conv_in = (first * second).astype(bf16).astype(f32)
        pad[HALO : HALO + rows, :] = conv_in
        total = w_taps[TAPS - 1 : TAPS] * conv_in
        for j in range(TAPS - 1):
            lo = HALO - (TAPS - 1) + j
            total += w_taps[j : j + 1] * pad[lo : lo + rows, :]
        conv_all[me, at, :] = per_group(proj_b * total, group_gain[...]).astype(bf16)

        @pl.when(t == 0)
        def _():
            head_conv[...] = conv_in[:HALO]
            head_gate[...] = proj_b[:HALO]
            start(own_copies(CONV, 0))

        @pl.when(t > 0)
        def _():
            start(own_copies(CONV, t))

        pad[0:HALO, :] = conv_in[rows - HALO :]

        @pl.when(t == nb - 1)
        def _():
            tail[...] = conv_in[rows - HALO :]

            @pl.when(leads)
            def _():
                pl.semaphore_wait(rim_ready, 1)

            @pl.when(place < sp - 1)
            def _():
                rim_copy.start()

            pass_mates(CONV)

        @pl.when(t == min(2, nb - 1))
        def _():
            for copy in twin_copies():
                copy.wait_recv()
            log_second = jnp.where(member == 0, peer_log[0:1, :], offset[0:1, :])
            decay = jnp.exp(log_second)
            for h in range(heads):
                own, other = state[h], peer_state[h].astype(f32)
                early = jnp.where(member == 0, own, other)
                late = jnp.where(member == 0, other, own)
                sent_total[h] = (early * decay[:, head_slice(h)] + late).astype(bf16)
            sent_log[0:1, :] = offset[0:1, :] + peer_log[0:1, :]

            @pl.when(pair < pairs - 1)
            def _():
                pl.semaphore_wait(ready, pairs - 1 - pair)

            for k in range(1, pairs):
                @pl.when(pair + k < pairs)
                def _():
                    start(total_copies(k, pair))

        return 0

    lax.fori_loop(0, nb, conv_block, 0)

    for n in (5, 6):
        weight_copy(n).wait()

    def read_block(t, _):
        at = block(t)
        both = dot(normed_all[at, :], w_read[...])
        query = jax.nn.silu(both[:, :width].astype(bf16).astype(f32))
        outgate = jax.nn.silu(both[:, width:].astype(bf16).astype(f32))
        for h in range(heads):
            s = head_slice(h)
            gate[at, s] = outgate[:, s] * state_gain[...]
        for b in range(rows // CHUNK):
            lo, hi = b * CHUNK, (b + 1) * CHUNK
            where = pl.ds(pl.multiple_of(t * rows + lo, CHUNK), CHUNK)
            number = t * (rows // CHUNK) + b
            cum = cums[where, :]
            mid = cum[CHUNK // 2 - 1 : CHUNK // 2]
            q_mid = query[lo:hi] * jnp.exp(cum - mid)
            q_all = q_mid * jnp.exp(mid)
            qdev[where, :] = (q_all * jnp.exp(offsets[number, 0:1, :])).astype(bf16)
            q_mid, q_all = q_mid.astype(bf16), q_all.astype(bf16)
            for h in range(heads):
                s = head_slice(h)
                scores = dot(q_mid[:, s], key_mid[where, s], ((1,), (1,)))
                scores = jnp.where(causal, scores, 0.0).astype(bf16)
                read[where, s] = dot(scores, value_all[where, s]) + dot(
                    q_all[:, s], olds[number, h], ((1,), (1,))
                )

        @pl.when(t == nb - 1)
        def _():
            @pl.when(place == 0)
            def _():
                rim[...] = jnp.zeros_like(rim)

            @pl.when(place > 0)
            def _():
                rim_copy.wait_recv()

            ext = jnp.concatenate([rim[...], head_conv[...]], axis=0)
            fixed = w_taps[TAPS - 1 : TAPS] * head_conv[...]
            for j in range(TAPS - 1):
                lo = HALO - (TAPS - 1) + j
                fixed += w_taps[j : j + 1] * ext[lo : lo + HALO]
            fixed = per_group(head_gate[...] * fixed, group_gain[...])
            conv_all[me, 0:HALO, :] = fixed.astype(bf16)
            start(own_copies(CONV, nb))
            pass_mates(MIX)

        return 0

    lax.fori_loop(0, nb, read_block, 0)

    for k in range(1, pairs):
        @pl.when(pair >= k)
        def _():
            for copy in total_copies(k, pair - k):
                copy.wait_recv()
    incoming[...] = jnp.zeros_like(incoming)

    def hop(p, _):
        decay = jnp.exp(total_logs[p, 0:1, :])
        for h in range(heads):
            incoming[h] = incoming[h] * decay[:, head_slice(h)] + totals[p, h].astype(f32)
        return 0

    lax.fori_loop(0, pair, hop, 0)
    decay = jnp.exp(peer_log[0:1, :])
    for h in range(heads):
        through = incoming[h] * decay[:, head_slice(h)] + peer_state[h].astype(f32)
        incoming[h] = jnp.where(member == 0, incoming[h], through)

    def merge(t, _):
        at = block(t)
        for h in range(heads):
            s = head_slice(h)
            whole = read[at, s] + dot(qdev[at, s], incoming[h].astype(bf16), ((1,), (1,)))
            mix_all[me, at, s] = (rms(whole) * gate[at, s]).astype(bf16)
        start(own_copies(MIX, t))
        return 0

    lax.fori_loop(0, nb, merge, 0)

    for kind in (CONV, MIX):
        own_columns(kind).wait()
        pair_columns(kind, partner).wait_recv()

    def near(kind, t):
        out = dot(held[kind][me, block(t), :], columns[kind, me])
        return out + dot(held[kind][partner, block(t), :], columns[kind, partner])

    def near_conv(t, _):
        acc_all[block(t), :] = near(CONV, t)
        return 0

    arrived(CONV, 0, partner)
    arrived(CONV, nb, partner)

    def conv_partner(t, _):
        arrived(CONV, t + 1, partner)
        return 0

    lax.fori_loop(0, nb - 1, conv_partner, 0)
    lax.fori_loop(0, nb, near_conv, 0)


    def near_mix(t, _):
        arrived(MIX, t, partner)
        acc_all[block(t), :] += near(MIX, t)
        return 0

    lax.fori_loop(0, nb, near_mix, 0)

    def conv_relay(t, _):
        relay(CONV, t + 1)
        return 0

    relay(CONV, 0)
    lax.fori_loop(0, nb - 1, conv_relay, 0)
    relay(CONV, nb)
    for kind in (CONV, MIX):
        for k, c in far_devices:
            for g in (mine + 1 - 2 * lax.rem(mine, 2), mates_piece + 1 - 2 * lax.rem(mine, 2)):
                piece_in(kind, far(k, c), g).wait_recv()
    for k in range(1, chips):
        arrived(CONV, 0, far(k, 1 - core))
        arrived(CONV, nb, far(k, 1 - core))

    def conv_arrivals(t, _):
        for k in range(1, chips):
            arrived(CONV, t + 1, far(k, 1 - core))
        return 0

    lax.fori_loop(0, nb - 1, conv_arrivals, 0)

    def far_conv(t, _):
        acc = acc_all[block(t), :]
        for k, c in far_devices:
            origin = far(k, c)
            acc += dot(conv_all[origin, block(t), :], columns[CONV, origin])
        acc_all[block(t), :] = acc
        return 0

    lax.fori_loop(0, nb, far_conv, 0)

    def finish(t, _):
        relay(MIX, t)
        for k in range(1, chips):
            arrived(MIX, t, far(k, 1 - core))
        acc = acc_all[block(t), :]
        for k, c in far_devices:
            origin = far(k, c)
            acc += dot(mix_all[origin, block(t), :], columns[MIX, origin])
        result[block(t), :] = acc.astype(bf16)
        return 0

    lax.fori_loop(0, nb, finish, 0)

    def drain(t, _):
        for copy in own_copies(MIX, t) + relays(MIX, t):
            copy.wait_send()
        return 0

    def drain_conv(t, _):
        for copy in own_copies(CONV, t + 1) + relays(CONV, t + 1):
            copy.wait_send()
        return 0

    lax.fori_loop(0, nb, drain, 0)
    lax.fori_loop(0, nb - 1, drain_conv, 0)
    for t in (0, nb):
        for copy in own_copies(CONV, t) + relays(CONV, t):
            copy.wait_send()
    for kind in (CONV, MIX):
        pair_columns(kind, me).wait_send()
        for k, c in far_devices:
            piece_out(kind, k, c).wait_send()
            for n in range(3):
                pass_on(kind, k, c, n).wait_send()

    @pl.when(place < sp - 1)
    def _():
        rim_copy.wait_send()

    for copy in twin_copies():
        copy.wait_send()
    for k in range(1, pairs):
        @pl.when(pair + k < pairs)
        def _():
            for copy in total_copies(k, pair):
                copy.wait_send()


def body(
    tokens, in_gain, w_query, w_forget, w_input, w_outgate, w_conv_h, w_conv_b, w_conv_c,
    forget_floor, forget_leak, state_gain, conv_taps, group_gain, out_state, out_conv,
):
    count, feats = tokens.shape
    width, channels = w_query.shape[1], w_conv_h.shape[1]
    heads = width // GROUP_FEATURES
    tp, sp = lax.axis_size("tp"), lax.axis_size("sp")
    ncols, nb, chips = out_state.shape[1] // tp, count // ROWS, tp // 2
    share = min(SHARE, sp)
    chunks, pairs = count // CHUNK, sp // 2

    hbm = pl.BlockSpec(memory_space=pltpu.HBM)
    vmem = pl.BlockSpec(memory_space=pltpu.VMEM)
    sems = pltpu.SemaphoreType.DMA
    square = (heads, GROUP_FEATURES, GROUP_FEATURES)
    return pl.pallas_call(
        functools.partial(fused_kernel, tp, sp, share),
        in_specs=[hbm, vmem] + [hbm] * 7 + [vmem, hbm, vmem, vmem, vmem, hbm, hbm],
        out_specs=vmem,
        out_shape=pltpu.VMEM((count, ncols), bf16),
        scratch_shapes=[
            pltpu.VMEM((count, feats), bf16),
            pltpu.VMEM((feats, 2 * width), bf16),
            pltpu.VMEM((feats, 3 * channels), bf16),
            pltpu.VMEM((feats, 2 * width), bf16),
            pltpu.VMEM((count, width), f32),
            pltpu.VMEM((count, width), bf16),
            pltpu.VMEM((count, width), bf16),
            pltpu.VMEM((chunks,) + square, bf16),
            pltpu.VMEM((chunks, HALO, width), f32),
            pltpu.VMEM((HALO + ROWS, channels), f32),
            pltpu.VMEM(square, f32),
            pltpu.VMEM((HALO, width), f32),
            pltpu.VMEM((count, width), f32),
            pltpu.VMEM((count, width), bf16),
            pltpu.VMEM((count, width), f32),
            pltpu.VMEM((tp, count, channels), bf16),
            pltpu.VMEM((tp, count, width), bf16),
            pltpu.VMEM((2, tp, width, ncols), bf16),
            pltpu.VMEM((count, ncols), f32),
            pltpu.VMEM(square, bf16),
            pltpu.VMEM(square, bf16),
            pltpu.VMEM((HALO, width), f32),
            pltpu.VMEM(square, bf16),
            pltpu.VMEM((HALO, width), f32),
            pltpu.VMEM((pairs,) + square, bf16),
            pltpu.VMEM((pairs, HALO, width), f32),
            pltpu.VMEM((HALO, channels), f32),
            pltpu.VMEM((HALO, channels), f32),
            pltpu.VMEM((HALO, channels), f32),
            pltpu.VMEM((HALO, channels), f32),
            pltpu.VMEM(square, f32),
            sems((nb,)), sems((nb,)), sems((7,)), sems((2,)),
            sems((2,)), sems((2,)), sems((2, chips, 2)), sems((2, tp, share)),
            sems((2, chips, 2, 3)),
            sems((2, chips, nb + 1)), sems((2, chips, nb + 1)), sems((2, tp, nb + 1)),
            sems((2,)), sems((2,)), sems((2, pairs)), sems((2, pairs)), sems((1,)), sems((1,)),
            pltpu.SemaphoreType.REGULAR, pltpu.SemaphoreType.REGULAR,
        ],
        compiler_params=pltpu.CompilerParams(
            vmem_limit_bytes=56 * 2**20, collective_id=0, has_side_effects=True
        ),
    )(
        tokens, in_gain[None], w_query, w_forget, w_input, w_outgate, w_conv_h, w_conv_b, w_conv_c,
        forget_floor[None], forget_leak, state_gain[None], conv_taps, group_gain[None],
        out_state, out_conv,
    )


def solution(mesh):
    cols, rows = P(None, "tp"), P("tp", None)
    in_specs = (
        P("sp", None), P(), cols, cols, cols, cols, cols, cols, cols,
        P("tp"), P("sp", "tp"), P(), cols, P(), rows, rows,
    )
    return jax.shard_map(
        body, mesh=mesh, in_specs=in_specs, out_specs=P("sp", "tp"), check_vma=False
    )
```

```python
import functools

import jax
import jax.numpy as jnp
from jax import lax
from jax.experimental import pallas as pl
from jax.experimental.pallas import tpu as pltpu
from jax.sharding import PartitionSpec as P

GROUP_FEATURES = 128
CHUNK = 128
ROWS = 256
MIX_ROWS = 128
LAG = 2
EXTRA = 16
TAPS = 3
HALO = 8
HEAD = 16
SHARE = 4
CONV, MIX = 0, 1

norm_eps = 1e-06
f32 = jnp.float32
bf16 = jnp.bfloat16


def dot(a, b, dims=((1,), (0,))):
    return lax.dot_general(a, b, (dims, ((), ())), preferred_element_type=f32)


def rms(values):
    return values * lax.rsqrt(jnp.mean(values * values, axis=-1, keepdims=True) + norm_eps)


def per_group(values, gain):
    parts = []
    for g in range(values.shape[1] // GROUP_FEATURES):
        parts.append(rms(values[:, g * GROUP_FEATURES : (g + 1) * GROUP_FEATURES]) * gain)
    return jnp.concatenate(parts, axis=1)


def head_slice(h):
    return slice(h * GROUP_FEATURES, (h + 1) * GROUP_FEATURES)


def prefix_sum(ones, values):
    high = values.astype(bf16)
    rest = values - high.astype(f32)
    middle = rest.astype(bf16)
    low = (rest - middle.astype(f32)).astype(bf16)
    return dot(ones, jnp.concatenate([high, middle, low], axis=0))


def fused_kernel(
    tp, sp, share,
    tokens, in_gain_in, wq, wf, wi, wg, wh, wb, wc, floor_in, leak, state_gain_in, taps_in,
    group_gain_in, out_state, out_conv, result,
    in_gain, floor, state_gain, taps, group_gain, small_sem,
    normed_all, w_scan, w_conv, w_read, cums, key_mid, value_all, olds, offsets,
    pad, state, offset, read, qdev, gate, conv_all, mix_all, columns, acc_all,
    sent_state, peer_state, sent_total, totals,
    rim, tail, head_conv, head_gate, incoming,
    tok_sem, leak_sem, w_sem, own_sem,
    pair_send, pair_recv, piece_send, piece_recv, mate_send,
    blk_send, fwd_send, conv_recv, mix_first, mix_recv, l1_send, l1_recv, l2_send, l2_recv, rim_send, rim_recv,
    ready, rim_ready, twin_ready, mate_ready,
):
    me, place = lax.axis_index("tp"), lax.axis_index("sp")
    partner = me + 1 - 2 * lax.rem(me, 2)
    chips = tp // 2
    chip = lax.div(me, 2)
    core = lax.rem(me, 2)
    count, feats = normed_all.shape
    width = value_all.shape[1]
    channels = pad.shape[1]
    rows = ROWS
    nb, mix_nb = count // rows, count // MIX_ROWS
    ncols = result.shape[1]
    heads = state.shape[0]
    piece = width // share
    mine = lax.rem(place, share)
    twin = place + 1 - 2 * lax.rem(place, 2)
    across = share // 2
    step = across - share * lax.div(mine, across)
    mate, mates_piece = place + step, mine + step
    member = lax.rem(place, 2)
    pair = lax.div(place, 2)
    pairs = sp // 2
    before, after = lax.rem(place + sp - 1, sp), lax.rem(place + 1, sp)
    held = (conv_all, mix_all)
    outs = (out_conv, out_state)

    def block(t):
        if isinstance(t, int):
            return pl.ds(t * rows, rows)
        return pl.ds(pl.multiple_of(t * rows, rows), rows)

    def mix_block(t):
        return pl.ds(pl.multiple_of(t * MIX_ROWS, MIX_ROWS), MIX_ROWS)

    def token_copy(t):
        return pltpu.make_async_copy(tokens.at[block(t)], normed_all.at[block(t)], tok_sem.at[t])

    def leak_copy(t):
        at = block(0) if t == 0 else pl.ds(rows, count - rows)
        return pltpu.make_async_copy(leak.at[at], cums.at[at], leak_sem.at[t])

    weights = ((wf, 0, 0), (wi, 0, 1), (wc, 1, 0), (wh, 1, 1), (wb, 1, 2), (wq, 2, 0), (wg, 2, 1))

    phases = [w_scan, w_conv, w_read]

    def weight_copy(n):
        src, phase, slot = weights[n]
        dst = phases[phase]
        return pltpu.make_async_copy(
            src, dst.at[:, slot * width : (slot + 1) * width], w_sem.at[phase]
        )

    def weight_wait(phase):
        dst = phases[phase]
        pltpu.make_async_copy(dst, dst, w_sem.at[phase]).wait()

    def cols_of(device):
        return pl.ds(pl.multiple_of(device * ncols, ncols), ncols)

    def piece_rows(g):
        return pl.ds(pl.multiple_of(g * piece, piece), piece)

    def own_columns(kind):
        return pltpu.make_async_copy(
            outs[kind].at[:, cols_of(me)], columns.at[kind, me], own_sem.at[0]
        )

    def pair_columns(kind, origin):
        return pltpu.make_async_remote_copy(
            outs[kind].at[:, cols_of(partner)], columns.at[kind, origin],
            pair_send.at[0], pair_recv.at[0], device_id={"tp": partner},
        )

    def far(k, c):
        return lax.rem(chip + k, chips) * 2 + c

    def piece_out(kind, k, c):
        target = far(k, c)
        return pltpu.make_async_remote_copy(
            outs[kind].at[piece_rows(mine), cols_of(target)],
            columns.at[kind, me, piece_rows(mine)],
            piece_send.at[kind, k - 1, c], piece_recv.at[kind, chips - k - 1, core, 0],
            device_id={"tp": target},
        )

    def piece_in(kind, k, c, n):
        size = (piece, piece, 2 * piece)[n]
        ref = columns.at[kind, me, 0:size]
        return pltpu.make_async_copy(ref, ref, piece_recv.at[kind, k - 1, c, n])

    def pass_on(kind, k, c, n):
        g, to = ((mine, mate), (mine, twin), (mates_piece, twin))[n]
        ref = columns.at[kind, far(k, c), piece_rows(g)]
        return pltpu.make_async_remote_copy(
            ref, ref, mate_send.at[kind, k - 1, c],
            piece_recv.at[kind, k - 1, c, (1, 2, 2)[n]], device_id={"sp": to},
        )

    def pass_own(kind):
        for k, c in far_devices:
            piece_in(kind, k, c, 0).wait()
            pass_on(kind, k, c, 0).start()
            pass_on(kind, k, c, 1).start()

    def pass_mates(kind):
        for k, c in far_devices:
            piece_in(kind, k, c, 1).wait()
            pass_on(kind, k, c, 2).start()

    far_devices = [(k, c) for k in range(1, chips) for c in range(2)]

    def span(kind, t):
        if kind == CONV and isinstance(t, int):
            if t == 0:
                return pl.ds(HEAD, rows - HEAD)
            if t == nb:
                return pl.ds(0, HEAD)
        return mix_block(t) if kind == MIX else block(t)

    def recv_sem(kind, slot, t):
        return conv_recv.at[slot] if kind == CONV or slot == 0 else mix_recv.at[slot - 1, t]

    def first_recv(kind):
        return (conv_recv if kind == CONV else mix_first).at[0]

    def own_copies(kind, t):
        ref = held[kind].at[me, span(kind, t)]
        out = []
        for k in range(1, chips):
            out.append(pltpu.make_async_remote_copy(
                ref, ref, blk_send.at[kind, k], recv_sem(kind, chips - k, t),
                device_id={"tp": far(k, core)},
            ))
        out.append(pltpu.make_async_remote_copy(
            ref, ref, blk_send.at[kind, 0], first_recv(kind), device_id={"tp": partner}
        ))
        return out

    def relays(kind, t):
        out = []
        for k in range(1, chips):
            ref = held[kind].at[far(k, core)]
            if kind == MIX:
                ref = ref.at[mix_block(t)]
            out.append(pltpu.make_async_remote_copy(
                ref, ref, fwd_send.at[kind, k - 1], recv_sem(kind, chips - 1 + k, t),
                device_id={"tp": partner},
            ))
        return out

    def start(copies):
        for copy in copies:
            copy.start()

    def landed(kind, slot, t):
        ref = held[kind].at[me]
        if kind == MIX:
            ref = ref.at[mix_block(t)]
        pltpu.make_async_copy(ref, ref, recv_sem(kind, slot, t)).wait()

    def relay(kind, t):
        for k, copy in enumerate(relays(kind, t)):
            landed(kind, k + 1, t)
            copy.start()

    def first_landed(kind):
        ref = held[kind].at[me]
        pltpu.make_async_copy(ref, ref, first_recv(kind)).wait()

    def sent(kind):
        ref = held[kind].at[me]
        for k in range(chips):
            pltpu.make_async_copy(ref, ref, blk_send.at[kind, k]).wait()

    def passed_on(kind):
        ref = held[kind].at[me]
        for k in range(1, chips):
            pltpu.make_async_copy(ref, ref, fwd_send.at[kind, k - 1]).wait()

    twin_copy = pltpu.make_async_remote_copy(
        sent_state, peer_state, l1_send.at[0], l1_recv.at[0], device_id={"sp": twin}
    )

    def total_copy(k, source):
        return pltpu.make_async_remote_copy(
            sent_total, totals.at[source], l2_send.at[k - 1], l2_recv.at[source],
            device_id={"sp": lax.rem(place + 2 * k, sp)},
        )

    def put_decay(ref, decay):
        high = decay.astype(bf16)
        low = (decay - high.astype(f32)).astype(bf16)
        for h in range(heads):
            s = head_slice(h)
            both = jnp.concatenate([high[:, s], low[:, s]], axis=0)
            both = jnp.concatenate([both] * (EXTRA // 2), axis=0)
            ref[h, GROUP_FEATURES:, :] = both

    def decay_of(rows_of):
        both = rows_of.astype(f32)
        return both[0:1] + both[1:2]

    rim_copy = pltpu.make_async_remote_copy(
        tail, rim, rim_send.at[0], rim_recv.at[0], device_id={"sp": after}
    )

    small = ((in_gain_in, in_gain), (floor_in, floor), (state_gain_in, state_gain),
             (taps_in, taps), (group_gain_in, group_gain))

    def small_copy(n):
        return pltpu.make_async_copy(small[n][0], small[n][1], small_sem.at[n])

    small_copy(0).start()
    token_copy(0).start()
    weight_copy(0).start()
    weight_copy(1).start()
    small_copy(1).start()
    leak_copy(0).start()
    if nb > 1:
        token_copy(1).start()
        leak_copy(1).start()
    barrier = pltpu.get_barrier_semaphore()
    for k in range(1, tp):
        pl.semaphore_signal(barrier, inc=1, device_id={"tp": lax.rem(me + k, tp)})
    for to, low in ((twin, member == 0), (mate, step > 0)):
        @pl.when(low)
        def _():
            pl.semaphore_signal(barrier, inc=1, device_id={"sp": to})

    for k in range(1, pairs):
        @pl.when(pair + k < pairs)
        def _():
            pl.semaphore_signal(barrier, inc=1, device_id={"sp": lax.rem(place + 2 * k, sp)})
    follows = jnp.logical_and(member == 0, pair > 0)
    leads = jnp.logical_and(member == 1, pair < pairs - 1)

    @pl.when(leads)
    def _():
        pl.semaphore_signal(barrier, inc=1, device_id={"sp": after})

    lower = pair + member + jnp.where(step > 0, 0, 1) + jnp.where(follows, 1, 0)
    pl.semaphore_wait(barrier, tp - 1 + lower)

    @pl.when(member == 1)
    def _():
        pl.semaphore_signal(twin_ready, inc=1, device_id={"sp": twin})

    @pl.when(step < 0)
    def _():
        pl.semaphore_signal(mate_ready, inc=1, device_id={"sp": mate})

    for k in range(1, pairs):
        @pl.when(pair >= k)
        def _():
            pl.semaphore_signal(ready, inc=1, device_id={"sp": lax.rem(place + sp - 2 * k, sp)})

    @pl.when(follows)
    def _():
        pl.semaphore_signal(rim_ready, inc=1, device_id={"sp": before})
    for kind in (CONV, MIX):
        for k, c in far_devices:
            piece_out(kind, k, c).start()
    for t in range(2, nb):
        token_copy(t).start()
    for n in (2, 3, 4):
        small_copy(n).start()
    for kind in (CONV, MIX):
        pair_columns(kind, me).start()
        own_columns(kind).start()

    state[...] = jnp.zeros_like(state)
    offset[...] = jnp.zeros_like(offset)
    pad[0:HALO, :] = jnp.zeros((HALO, channels), f32)

    r = lax.broadcasted_iota(jnp.int32, (CHUNK, CHUNK), 0)
    c = lax.broadcasted_iota(jnp.int32, (CHUNK, CHUNK), 1)
    causal = r >= c
    ones = jnp.concatenate([causal.astype(f32)] * 3, axis=1).astype(bf16)

    def arrive(t):
        token_copy(t).wait()
        if t < 2:
            leak_copy(t).wait()

    def norm(t):
        arrive(t)
        normalize(t)

    def normalize(t):
        at = block(t)
        normed_all[at, :] = (rms(normed_all[at, :].astype(f32)) * in_gain[...]).astype(bf16)

    def scan_product(t):
        return dot(normed_all[block(t), :], w_scan[...])

    def scan_block(t, both):
        at = block(t)
        x = both[:, :width].astype(bf16).astype(f32)
        value = both[:, width:].astype(bf16)
        value_all[at, :] = value
        key = (1.0 - floor[...]) * jax.nn.sigmoid(-x)
        logf = jnp.log(1.0 - key) + cums[at, :]
        for b in range(rows // CHUNK):
            lo, hi = b * CHUNK, (b + 1) * CHUNK
            where = pl.ds(t * rows + lo, CHUNK)
            number = t * (rows // CHUNK) + b
            cum = prefix_sum(ones, logf[lo:hi])
            mid = cum[CHUNK // 2 - 1 : CHUNK // 2]
            last = cum[CHUNK - 1 : CHUNK]
            k_mid = key[lo:hi] * jnp.exp(mid - cum)
            k_end = (k_mid * jnp.exp(last - mid)).astype(bf16)
            cums[where, :] = cum
            key_mid[where, :] = k_mid.astype(bf16)
            offsets[number] = offset[...]
            for h in range(heads):
                s = head_slice(h)
                old = state[h]
                olds[number, h] = old.astype(bf16)
                state[h] = old * jnp.exp(last[:, s]) + dot(
                    value[lo:hi, s], k_end[:, s], ((0,), (0,))
                )
            offset[...] += last

    small_copy(0).wait()
    norm(0)
    small_copy(1).wait()
    weight_wait(0)
    for n in range(2, 7):
        weight_copy(n).start()
    product = scan_product(0)
    if nb > 1:
        norm(1)
    for t in range(nb):
        if t + 2 < nb:
            arrive(t + 2)
        if t + 1 < nb:
            later = scan_product(t + 1)
        if t + 2 < nb:
            normalize(t + 2)
        scan_block(t, product)
        product = later
    sent_state[:, :GROUP_FEATURES, :] = state[...].astype(bf16)
    put_decay(sent_state, jnp.exp(offset[0:1, :]))

    @pl.when(member == 0)
    def _():
        pl.semaphore_wait(twin_ready, 1)

    twin_copy.start()

    @pl.when(step > 0)
    def _():
        pl.semaphore_wait(mate_ready, 1)

    pass_own(CONV)

    weight_wait(1)
    for n in (2, 3, 4):
        small_copy(n).wait()
    w_taps = taps[...].astype(f32)

    def conv_product(t):
        return dot(normed_all[block(t), :], w_conv[...])

    def conv_block(t, three):
        at = block(t)
        first = three[:, :channels].astype(bf16).astype(f32)
        second = three[:, channels : 2 * channels].astype(bf16).astype(f32)
        proj_b = three[:, 2 * channels :].astype(bf16).astype(f32)
        conv_in = (first * second).astype(bf16).astype(f32)
        pad[HALO : HALO + rows, :] = conv_in
        total = w_taps[TAPS - 1 : TAPS] * conv_in
        for j in range(TAPS - 1):
            lo = HALO - (TAPS - 1) + j
            total += w_taps[j : j + 1] * pad[lo : lo + rows, :]
        conv_all[me, at, :] = per_group(proj_b * total, group_gain[...]).astype(bf16)

        @pl.when(t == 0)
        def _():
            head_conv[...] = conv_in[:HALO]
            head_gate[...] = proj_b[:HALO]
            start(own_copies(CONV, 0))

        @pl.when(t > 0)
        def _():
            start(own_copies(CONV, t))

        pad[0:HALO, :] = conv_in[rows - HALO :]

        @pl.when(t == nb - 1)
        def _():
            tail[...] = conv_in[rows - HALO :]

            @pl.when(leads)
            def _():
                pl.semaphore_wait(rim_ready, 1)

            @pl.when(place < sp - 1)
            def _():
                rim_copy.start()

            pass_mates(CONV)

        @pl.when(t == min(2, nb - 1))
        def _():
            twin_copy.wait_recv()
            decays = []
            for h in range(heads):
                s = head_slice(h)
                own, other = state[h], peer_state[h, :GROUP_FEATURES, :].astype(f32)
                own_decay = jnp.exp(offset[0:1, s])
                peer_decay = decay_of(peer_state[h, GROUP_FEATURES:, :])
                early = jnp.where(member == 0, own, other)
                late = jnp.where(member == 0, other, own)
                decay = jnp.where(member == 0, peer_decay, own_decay)
                sent_total[h, :GROUP_FEATURES, :] = (early * decay + late).astype(bf16)
                decays.append(own_decay * peer_decay)
            put_decay(sent_total, jnp.concatenate(decays, axis=1))

            @pl.when(pair < pairs - 1)
            def _():
                pl.semaphore_wait(ready, pairs - 1 - pair)

            for k in range(1, pairs):
                @pl.when(pair + k < pairs)
                def _():
                    total_copy(k, pair).start()

    product = conv_product(0)
    for t in range(nb):
        if t + 1 < nb:
            later = conv_product(t + 1)
        conv_block(t, product)
        product = later

    weight_wait(2)

    def read_product(t):
        return dot(normed_all[block(t), :], w_read[...])

    def read_block(t, both):
        at = block(t)
        query = jax.nn.silu(both[:, :width].astype(bf16).astype(f32))
        outgate = jax.nn.silu(both[:, width:].astype(bf16).astype(f32))
        for h in range(heads):
            s = head_slice(h)
            gate[at, s] = outgate[:, s] * state_gain[...]
        for b in range(rows // CHUNK):
            lo, hi = b * CHUNK, (b + 1) * CHUNK
            where = pl.ds(t * rows + lo, CHUNK)
            number = t * (rows // CHUNK) + b
            cum = cums[where, :]
            mid = cum[CHUNK // 2 - 1 : CHUNK // 2]
            q_mid = query[lo:hi] * jnp.exp(cum - mid)
            q_all = q_mid * jnp.exp(mid)
            qdev[where, :] = (q_all * jnp.exp(offsets[number, 0:1, :])).astype(bf16)
            q_mid, q_all = q_mid.astype(bf16), q_all.astype(bf16)
            for h in range(heads):
                s = head_slice(h)
                scores = dot(q_mid[:, s], key_mid[where, s], ((1,), (1,)))
                scores = jnp.where(causal, scores, 0.0).astype(bf16)
                read[where, s] = dot(scores, value_all[where, s]) + dot(
                    q_all[:, s], olds[number, h], ((1,), (1,))
                )

        @pl.when(t == nb - 1)
        def _():
            @pl.when(place == 0)
            def _():
                rim[...] = jnp.zeros_like(rim)

            @pl.when(place > 0)
            def _():
                rim_copy.wait_recv()

            ext = jnp.concatenate([rim[...], head_conv[...]], axis=0)
            fixed = w_taps[TAPS - 1 : TAPS] * head_conv[...]
            for j in range(TAPS - 1):
                lo = HALO - (TAPS - 1) + j
                fixed += w_taps[j : j + 1] * ext[lo : lo + HALO]
            fixed = per_group(head_gate[...] * fixed, group_gain[...])
            conv_all[me, 0:HALO, :] = fixed.astype(bf16)
            start(own_copies(CONV, nb))

    product = read_product(0)
    for t in range(nb):
        if t + 1 < nb:
            later = read_product(t + 1)
        read_block(t, product)
        product = later

    for k in range(1, pairs):
        @pl.when(pair >= k)
        def _():
            total_copy(k, pair - k).wait_recv()
    incoming[...] = jnp.zeros_like(incoming)

    def hop(p, _):
        for h in range(heads):
            decay = decay_of(totals[p, h, GROUP_FEATURES:, :])
            incoming[h] = incoming[h] * decay + totals[p, h, :GROUP_FEATURES, :].astype(f32)
        return 0

    lax.fori_loop(0, pair, hop, 0)
    for h in range(heads):
        decay = decay_of(peer_state[h, GROUP_FEATURES:, :])
        through = incoming[h] * decay + peer_state[h, :GROUP_FEATURES, :].astype(f32)
        incoming[h] = jnp.where(member == 0, incoming[h], through)

    def merge(t, _):
        at = block(t)
        for h in range(heads):
            s = head_slice(h)
            whole = read[at, s] + dot(qdev[at, s], incoming[h].astype(bf16), ((1,), (1,)))
            mix_all[me, at, s] = (rms(whole) * gate[at, s]).astype(bf16)
        for n in range(rows // MIX_ROWS):
            start(own_copies(MIX, t * (rows // MIX_ROWS) + n))
        return 0

    lax.fori_loop(0, nb, merge, 0)
    pass_own(MIX)

    mine_both, pair_both = columns.at[:, me], columns.at[:, partner]
    pltpu.make_async_copy(mine_both, mine_both, own_sem.at[0]).wait()
    pltpu.make_async_copy(pair_both, pair_both, pair_recv.at[0]).wait()

    def near(kind, t):
        out = dot(held[kind][me, block(t), :], columns[kind, me])
        return out + dot(held[kind][partner, block(t), :], columns[kind, partner])

    def near_conv(t, _):
        acc_all[block(t), :] = near(CONV, t)
        return 0

    first_landed(CONV)
    lax.fori_loop(0, nb, near_conv, 0)


    def near_mix(t, _):
        acc_all[block(t), :] += near(MIX, t)
        return 0

    first_landed(MIX)
    lax.fori_loop(0, nb, near_mix, 0)

    pass_mates(MIX)

    relay(CONV, 0)
    for kind in (CONV, MIX):
        for k, c in far_devices:
            piece_in(kind, k, c, 2).wait()
    for k in range(1, chips):
        landed(CONV, chips - 1 + k, 0)

    def far_conv(t, _):
        acc = acc_all[block(t), :]
        for k, c in far_devices:
            origin = far(k, c)
            acc += dot(conv_all[origin, block(t), :], columns[CONV, origin])
        acc_all[block(t), :] = acc
        return 0

    lax.fori_loop(0, nb, far_conv, 0)

    sent(CONV)
    passed_on(CONV)
    for kind in (CONV, MIX):
        for k, c in far_devices:
            piece_out(kind, k, c).wait_send()
            passed = columns.at[kind, me, 0 : 3 * piece]
            pltpu.make_async_copy(passed, passed, mate_send.at[kind, k - 1, c]).wait()
    pltpu.make_async_copy(mine_both, mine_both, pair_send.at[0]).wait()

    @pl.when(place < sp - 1)
    def _():
        rim_copy.wait_send()

    twin_copy.wait_send()
    for k in range(1, pairs):
        @pl.when(pair + k < pairs)
        def _():
            total_copy(k, pair).wait_send()

    def finish(t, _):
        @pl.when(t + LAG < mix_nb)
        def _():
            relay(MIX, t + LAG)

        for k in range(1, chips):
            landed(MIX, chips - 1 + k, t)
        at = mix_block(t)
        acc = acc_all[at, :]
        for k, c in far_devices:
            origin = far(k, c)
            acc += dot(mix_all[origin, at, :], columns[MIX, origin])
        result[at, :] = acc.astype(bf16)
        return 0

    for t in range(min(LAG, mix_nb)):
        relay(MIX, t)
    lax.fori_loop(0, mix_nb, finish, 0)

    sent(MIX)
    passed_on(MIX)


def body(
    tokens, in_gain, w_query, w_forget, w_input, w_outgate, w_conv_h, w_conv_b, w_conv_c,
    forget_floor, forget_leak, state_gain, conv_taps, group_gain, out_state, out_conv,
):
    count, feats = tokens.shape
    width, channels = w_query.shape[1], w_conv_h.shape[1]
    heads = width // GROUP_FEATURES
    tp, sp = lax.axis_size("tp"), lax.axis_size("sp")
    ncols, nb, chips = out_state.shape[1] // tp, count // ROWS, tp // 2
    share = min(SHARE, sp)
    chunks, pairs = count // CHUNK, sp // 2

    hbm = pl.BlockSpec(memory_space=pltpu.HBM)
    vmem = pl.BlockSpec(memory_space=pltpu.VMEM)
    sems = pltpu.SemaphoreType.DMA
    square = (heads, GROUP_FEATURES, GROUP_FEATURES)
    longer = (heads, GROUP_FEATURES + EXTRA, GROUP_FEATURES)
    return pl.pallas_call(
        functools.partial(fused_kernel, tp, sp, share),
        in_specs=[hbm] * 16,
        out_specs=vmem,
        out_shape=pltpu.VMEM((count, ncols), bf16),
        scratch_shapes=[
            pltpu.VMEM((1, feats), f32),
            pltpu.VMEM((1, width), f32),
            pltpu.VMEM((1, GROUP_FEATURES), f32),
            pltpu.VMEM((TAPS, channels), bf16),
            pltpu.VMEM((1, GROUP_FEATURES), f32),
            sems((5,)),
            pltpu.VMEM((count, feats), bf16),
            pltpu.VMEM((feats, 2 * width), bf16),
            pltpu.VMEM((feats, 3 * channels), bf16),
            pltpu.VMEM((feats, 2 * width), bf16),
            pltpu.VMEM((count, width), f32),
            pltpu.VMEM((count, width), bf16),
            pltpu.VMEM((count, width), bf16),
            pltpu.VMEM((chunks,) + square, bf16),
            pltpu.VMEM((chunks, HALO, width), f32),
            pltpu.VMEM((HALO + ROWS, channels), f32),
            pltpu.VMEM(square, f32),
            pltpu.VMEM((HALO, width), f32),
            pltpu.VMEM((count, width), f32),
            pltpu.VMEM((count, width), bf16),
            pltpu.VMEM((count, width), f32),
            pltpu.VMEM((tp, count, channels), bf16),
            pltpu.VMEM((tp, count, width), bf16),
            pltpu.VMEM((2, tp, width, ncols), bf16),
            pltpu.VMEM((count, ncols), f32),
            pltpu.VMEM(longer, bf16),
            pltpu.VMEM(longer, bf16),
            pltpu.VMEM(longer, bf16),
            pltpu.VMEM((pairs,) + longer, bf16),
            pltpu.VMEM((HALO, channels), f32),
            pltpu.VMEM((HALO, channels), f32),
            pltpu.VMEM((HALO, channels), f32),
            pltpu.VMEM((HALO, channels), f32),
            pltpu.VMEM(square, f32),
            sems((nb,)), sems((2,)), sems((3,)), sems((1,)),
            sems((1,)), sems((1,)), sems((2, chips - 1, 2)), sems((2, chips - 1, 2, 3)),
            sems((2, chips - 1, 2)),
            sems((2, chips)), sems((2, chips - 1)), sems((2 * chips - 1,)), sems((1,)),
            sems((2 * chips - 2, count // MIX_ROWS)),
            sems((1,)), sems((1,)), sems((pairs - 1,)), sems((pairs,)), sems((1,)), sems((1,)),
        ] + [pltpu.SemaphoreType.REGULAR] * 4,
        compiler_params=pltpu.CompilerParams(
            vmem_limit_bytes=56 * 2**20, collective_id=0, has_side_effects=True
        ),
    )(
        tokens, in_gain[None], w_query, w_forget, w_input, w_outgate, w_conv_h, w_conv_b, w_conv_c,
        forget_floor[None], forget_leak, state_gain[None], conv_taps, group_gain[None],
        out_state, out_conv,
    )


def solution(mesh):
    cols, rows = P(None, "tp"), P("tp", None)
    in_specs = (
        P("sp", None), P(), cols, cols, cols, cols, cols, cols, cols,
        P("tp"), P("sp", "tp"), P(), cols, P(), rows, rows,
    )
    return jax.shard_map(
        body, mesh=mesh, in_specs=in_specs, out_specs=P("sp", "tp"), check_vma=False
    )
```

```python
import functools

import jax
import jax.numpy as jnp
from jax import lax
from jax.experimental import pallas as pl
from jax.experimental.pallas import tpu as pltpu
from jax.sharding import PartitionSpec as P

GROUP_FEATURES = 128
CHUNK = 128
ROWS = 256
MIX_ROWS = 128
LAG = 2
EXTRA = 16
TAPS = 3
HALO = 8
HEAD = 16
SHARE = 4
CONV, MIX = 0, 1

norm_eps = 1e-06
f32 = jnp.float32
bf16 = jnp.bfloat16


def dot(a, b, dims=((1,), (0,))):
    return lax.dot_general(a, b, (dims, ((), ())), preferred_element_type=f32)


def rms(values):
    return values * lax.rsqrt(jnp.mean(values * values, axis=-1, keepdims=True) + norm_eps)


def per_group(values, gain):
    parts = []
    for g in range(values.shape[1] // GROUP_FEATURES):
        parts.append(rms(values[:, g * GROUP_FEATURES : (g + 1) * GROUP_FEATURES]) * gain)
    return jnp.concatenate(parts, axis=1)


def head_slice(h):
    return slice(h * GROUP_FEATURES, (h + 1) * GROUP_FEATURES)


def prefix_sum(ones, values):
    high = values.astype(bf16)
    rest = values - high.astype(f32)
    middle = rest.astype(bf16)
    low = (rest - middle.astype(f32)).astype(bf16)
    return dot(ones, jnp.concatenate([high, middle, low], axis=0))


def fused_kernel(
    tp, sp, share,
    tokens, in_gain_in, wq, wf, wi, wg, wh, wb, wc, floor_in, leak, state_gain_in, taps_in,
    group_gain_in, out_state, out_conv, result,
    in_gain, floor, state_gain, taps, group_gain, small_sem,
    normed_all, w_scan, w_conv, w_read, cums, key_mid, value_all, olds, offsets,
    pad, state, offset, read, qdev, gate, conv_all, mix_all, columns, acc_all,
    sent_state, peer_state, sent_total, totals,
    rim, tail, head_conv, head_gate, incoming,
    tok_sem, leak_sem, w_sem, own_sem,
    pair_send, pair_recv, piece_send, piece_recv, mate_send,
    blk_send, fwd_send, conv_recv, mix_first, mix_recv, l1_send, l1_recv, l2_send, l2_recv, rim_send, rim_recv,
    ready, rim_ready, twin_ready, mate_ready,
):
    me, place = lax.axis_index("tp"), lax.axis_index("sp")
    partner = me + 1 - 2 * lax.rem(me, 2)
    chips = tp // 2
    chip = lax.div(me, 2)
    core = lax.rem(me, 2)
    count, feats = normed_all.shape
    width = value_all.shape[1]
    channels = pad.shape[1]
    rows = ROWS
    nb, mix_nb = count // rows, count // MIX_ROWS
    ncols = result.shape[1]
    heads = state.shape[0]
    piece = width // share
    mine = lax.rem(place, share)
    twin = place + 1 - 2 * lax.rem(place, 2)
    across = share // 2
    step = across - share * lax.div(mine, across)
    mate, mates_piece = place + step, mine + step
    member = lax.rem(place, 2)
    pair = lax.div(place, 2)
    pairs = sp // 2
    before, after = lax.rem(place + sp - 1, sp), lax.rem(place + 1, sp)
    held = (conv_all, mix_all)
    outs = (out_conv, out_state)

    def block(t):
        if isinstance(t, int):
            return pl.ds(t * rows, rows)
        return pl.ds(pl.multiple_of(t * rows, rows), rows)

    def mix_block(t):
        return pl.ds(pl.multiple_of(t * MIX_ROWS, MIX_ROWS), MIX_ROWS)

    def token_copy(t):
        return pltpu.make_async_copy(tokens.at[block(t)], normed_all.at[block(t)], tok_sem.at[t])

    def leak_copy(t):
        at = block(0) if t == 0 else pl.ds(rows, count - rows)
        return pltpu.make_async_copy(leak.at[at], cums.at[at], leak_sem.at[t])

    weights = ((wf, 0, 0), (wi, 0, 1), (wc, 1, 0), (wh, 1, 1), (wb, 1, 2), (wq, 2, 0), (wg, 2, 1))
    weight_sems = (0, 0, 1, 2, 3, 4, 4)

    phases = [w_scan, w_conv, w_read]

    def weight_copy(n):
        src, phase, slot = weights[n]
        dst = phases[phase]
        return pltpu.make_async_copy(
            src, dst.at[:, slot * width : (slot + 1) * width], w_sem.at[weight_sems[n]]
        )

    def weight_wait(phase):
        dst = phases[phase]
        pltpu.make_async_copy(dst, dst, w_sem.at[weight_sems[2 * phase + phase // 2]]).wait()

    def cols_of(device):
        return pl.ds(pl.multiple_of(device * ncols, ncols), ncols)

    def piece_rows(g):
        return pl.ds(pl.multiple_of(g * piece, piece), piece)

    def own_columns(kind):
        return pltpu.make_async_copy(
            outs[kind].at[:, cols_of(me)], columns.at[kind, me], own_sem.at[0]
        )

    def pair_columns(kind, origin):
        return pltpu.make_async_remote_copy(
            outs[kind].at[:, cols_of(partner)], columns.at[kind, origin],
            pair_send.at[0], pair_recv.at[0], device_id={"tp": partner},
        )

    def far(k, c):
        return lax.rem(chip + k, chips) * 2 + c

    def piece_out(kind, k, c):
        target = far(k, c)
        return pltpu.make_async_remote_copy(
            outs[kind].at[piece_rows(mine), cols_of(target)],
            columns.at[kind, me, piece_rows(mine)],
            piece_send.at[kind, k - 1, c], piece_recv.at[kind, chips - k - 1, core, 0],
            device_id={"tp": target},
        )

    def piece_in(kind, k, c, n):
        size = (piece, piece, 2 * piece)[n]
        ref = columns.at[kind, me, 0:size]
        return pltpu.make_async_copy(ref, ref, piece_recv.at[kind, k - 1, c, n])

    def pass_on(kind, k, c, n):
        g, to = ((mine, mate), (mine, twin), (mates_piece, twin))[n]
        ref = columns.at[kind, far(k, c), piece_rows(g)]
        return pltpu.make_async_remote_copy(
            ref, ref, mate_send.at[kind, k - 1, c],
            piece_recv.at[kind, k - 1, c, (1, 2, 2)[n]], device_id={"sp": to},
        )

    def pass_own(kind, wait, which):
        for k, c in far_devices:
            if wait:
                piece_in(kind, k, c, 0).wait()
            for n in which:
                pass_on(kind, k, c, n).start()

    def pass_mates(kind):
        for k, c in far_devices:
            piece_in(kind, k, c, 1).wait()
            pass_on(kind, k, c, 2).start()

    far_devices = [(k, c) for k in range(1, chips) for c in range(2)]

    def span(kind, t):
        if kind == CONV and isinstance(t, int):
            if t == 0:
                return pl.ds(HEAD, rows - HEAD)
            if t == nb:
                return pl.ds(0, HEAD)
        return mix_block(t) if kind == MIX else block(t)

    def recv_sem(kind, slot, t):
        return conv_recv.at[slot] if kind == CONV or slot == 0 else mix_recv.at[slot - 1, t]

    def first_recv(kind):
        return (conv_recv if kind == CONV else mix_first).at[0]

    def own_copies(kind, t):
        ref = held[kind].at[me, span(kind, t)]
        out = []
        for k in range(1, chips):
            out.append(pltpu.make_async_remote_copy(
                ref, ref, blk_send.at[kind, k], recv_sem(kind, chips - k, t),
                device_id={"tp": far(k, core)},
            ))
        out.append(pltpu.make_async_remote_copy(
            ref, ref, blk_send.at[kind, 0], first_recv(kind), device_id={"tp": partner}
        ))
        return out

    def relays(kind, t):
        out = []
        for k in range(1, chips):
            ref = held[kind].at[far(k, core)]
            if kind == MIX:
                ref = ref.at[mix_block(t)]
            out.append(pltpu.make_async_remote_copy(
                ref, ref, fwd_send.at[kind, k - 1], recv_sem(kind, chips - 1 + k, t),
                device_id={"tp": partner},
            ))
        return out

    def start(copies):
        for copy in copies:
            copy.start()

    def landed(kind, slot, t):
        ref = held[kind].at[me]
        if kind == MIX:
            ref = ref.at[mix_block(t)]
        pltpu.make_async_copy(ref, ref, recv_sem(kind, slot, t)).wait()

    def relay(kind, t):
        for k, copy in enumerate(relays(kind, t)):
            landed(kind, k + 1, t)
            copy.start()

    def first_landed(kind):
        ref = held[kind].at[me]
        pltpu.make_async_copy(ref, ref, first_recv(kind)).wait()

    def sent(kind):
        ref = held[kind].at[me]
        for k in range(chips):
            pltpu.make_async_copy(ref, ref, blk_send.at[kind, k]).wait()

    def passed_on(kind):
        ref = held[kind].at[me]
        for k in range(1, chips):
            pltpu.make_async_copy(ref, ref, fwd_send.at[kind, k - 1]).wait()

    def twin_copy(h):
        return pltpu.make_async_remote_copy(
            sent_state.at[h], peer_state.at[h], l1_send.at[h], l1_recv.at[h],
            device_id={"sp": twin},
        )

    def total_copy(k, source, h):
        return pltpu.make_async_remote_copy(
            sent_total.at[h], totals.at[source, h], l2_send.at[h, k - 1], l2_recv.at[h, source],
            device_id={"sp": lax.rem(place + 2 * k, sp)},
        )

    def put_decay(ref, h, decay):
        high = decay.astype(bf16)
        low = (decay - high.astype(f32)).astype(bf16)
        both = jnp.concatenate([high, low], axis=0)
        ref[h, GROUP_FEATURES:, :] = jnp.concatenate([both] * (EXTRA // 2), axis=0)

    def decay_of(rows_of):
        both = rows_of.astype(f32)
        return both[0:1] + both[1:2]

    rim_copy = pltpu.make_async_remote_copy(
        tail, rim, rim_send.at[0], rim_recv.at[0], device_id={"sp": after}
    )

    small = ((in_gain_in, in_gain), (floor_in, floor), (state_gain_in, state_gain),
             (taps_in, taps), (group_gain_in, group_gain))

    def small_copy(n):
        return pltpu.make_async_copy(small[n][0], small[n][1], small_sem.at[n])

    small_copy(0).start()
    token_copy(0).start()
    weight_copy(0).start()
    weight_copy(1).start()
    small_copy(1).start()
    leak_copy(0).start()
    if nb > 1:
        token_copy(1).start()
        leak_copy(1).start()
    barrier = pltpu.get_barrier_semaphore()
    for k in range(1, tp):
        pl.semaphore_signal(barrier, inc=1, device_id={"tp": lax.rem(me + k, tp)})
    for to, low in ((twin, member == 0), (mate, step > 0)):
        @pl.when(low)
        def _():
            pl.semaphore_signal(barrier, inc=1, device_id={"sp": to})

    for k in range(1, pairs):
        @pl.when(pair + k < pairs)
        def _():
            pl.semaphore_signal(barrier, inc=1, device_id={"sp": lax.rem(place + 2 * k, sp)})
    follows = jnp.logical_and(member == 0, pair > 0)
    leads = jnp.logical_and(member == 1, pair < pairs - 1)

    @pl.when(leads)
    def _():
        pl.semaphore_signal(barrier, inc=1, device_id={"sp": after})

    lower = pair + member + jnp.where(step > 0, 0, 1) + jnp.where(follows, 1, 0)
    pl.semaphore_wait(barrier, tp - 1 + lower)

    @pl.when(member == 1)
    def _():
        pl.semaphore_signal(twin_ready, inc=1, device_id={"sp": twin})

    @pl.when(step < 0)
    def _():
        pl.semaphore_signal(mate_ready, inc=1, device_id={"sp": mate})

    for k in range(1, pairs):
        @pl.when(pair >= k)
        def _():
            pl.semaphore_signal(ready, inc=1, device_id={"sp": lax.rem(place + sp - 2 * k, sp)})

    @pl.when(follows)
    def _():
        pl.semaphore_signal(rim_ready, inc=1, device_id={"sp": before})
    for kind in (CONV, MIX):
        for k, c in far_devices:
            piece_out(kind, k, c).start()
    for t in range(2, nb):
        token_copy(t).start()
    for n in (2, 3, 4):
        small_copy(n).start()
    for kind in (CONV, MIX):
        pair_columns(kind, me).start()
        own_columns(kind).start()

    state[...] = jnp.zeros_like(state)
    offset[...] = jnp.zeros_like(offset)
    pad[0:HALO, :] = jnp.zeros((HALO, channels), f32)

    r = lax.broadcasted_iota(jnp.int32, (CHUNK, CHUNK), 0)
    c = lax.broadcasted_iota(jnp.int32, (CHUNK, CHUNK), 1)
    causal = r >= c
    ones = jnp.concatenate([causal.astype(f32)] * 3, axis=1).astype(bf16)

    def arrive(t):
        token_copy(t).wait()
        if t < 2:
            leak_copy(t).wait()

    def norm(t):
        arrive(t)
        normalize(t)

    def normalize(t):
        at = block(t)
        normed_all[at, :] = (rms(normed_all[at, :].astype(f32)) * in_gain[...]).astype(bf16)

    def scan_product(t):
        return dot(normed_all[block(t), :], w_scan[...])

    def scan_block(t, both):
        at = block(t)
        x = both[:, :width].astype(bf16).astype(f32)
        value = both[:, width:].astype(bf16)
        value_all[at, :] = value
        key = (1.0 - floor[...]) * jax.nn.sigmoid(-x)
        logf = jnp.log(1.0 - key) + cums[at, :]
        for b in range(rows // CHUNK):
            lo, hi = b * CHUNK, (b + 1) * CHUNK
            where = pl.ds(t * rows + lo, CHUNK)
            number = t * (rows // CHUNK) + b
            cum = prefix_sum(ones, logf[lo:hi])
            mid = cum[CHUNK // 2 - 1 : CHUNK // 2]
            last = cum[CHUNK - 1 : CHUNK]
            k_mid = key[lo:hi] * jnp.exp(mid - cum)
            k_end = (k_mid * jnp.exp(last - mid)).astype(bf16)
            cums[where, :] = cum
            key_mid[where, :] = k_mid.astype(bf16)
            offsets[number] = offset[...]
            for h in range(heads):
                s = head_slice(h)
                old = state[h]
                olds[number, h] = old.astype(bf16)
                state[h] = old * jnp.exp(last[:, s]) + dot(
                    value[lo:hi, s], k_end[:, s], ((0,), (0,))
                )
            offset[...] += last

    def conv_third(n):
        return dot(normed_all[block(0), :], w_conv[:, n * channels : (n + 1) * channels])


    def conv_product(t):
        return dot(normed_all[block(t), :], w_conv[...])

    def conv_block(t, three):
        at = block(t)
        first = three[:, :channels].astype(bf16).astype(f32)
        second = three[:, channels : 2 * channels].astype(bf16).astype(f32)
        proj_b = three[:, 2 * channels :].astype(bf16).astype(f32)
        conv_in = (first * second).astype(bf16).astype(f32)
        w_taps = taps[...].astype(f32)
        pad[HALO : HALO + rows, :] = conv_in
        total = w_taps[TAPS - 1 : TAPS] * conv_in
        for j in range(TAPS - 1):
            lo = HALO - (TAPS - 1) + j
            total += w_taps[j : j + 1] * pad[lo : lo + rows, :]
        conv_all[me, at, :] = per_group(proj_b * total, group_gain[...]).astype(bf16)

        @pl.when(t == 0)
        def _():
            head_conv[...] = conv_in[:HALO]
            head_gate[...] = proj_b[:HALO]
            start(own_copies(CONV, 0))

        @pl.when(t > 0)
        def _():
            start(own_copies(CONV, t))

        pad[0:HALO, :] = conv_in[rows - HALO :]

        @pl.when(t == nb - 1)
        def _():
            tail[...] = conv_in[rows - HALO :]

            @pl.when(leads)
            def _():
                pl.semaphore_wait(rim_ready, 1)

            @pl.when(place < sp - 1)
            def _():
                rim_copy.start()

            pass_own(MIX, True, (1,))

            @pl.when(step < 0)
            def _():
                pass_own(MIX, False, (0,))


        @pl.when(t == nb - 1)
        def _():
            @pl.when(pair < pairs - 1)
            def _():
                pl.semaphore_wait(ready, pairs - 1 - pair)

            for h in range(heads):
                s = head_slice(h)
                twin_copy(h).wait_recv()
                own, other = state[h], peer_state[h, :GROUP_FEATURES, :].astype(f32)
                own_decay = jnp.exp(offset[0:1, s])
                peer_decay = decay_of(peer_state[h, GROUP_FEATURES:, :])
                early = jnp.where(member == 0, own, other)
                late = jnp.where(member == 0, other, own)
                decay = jnp.where(member == 0, peer_decay, own_decay)
                sent_total[h, :GROUP_FEATURES, :] = (early * decay + late).astype(bf16)
                put_decay(sent_total, h, own_decay * peer_decay)
                for k in range(1, pairs):
                    @pl.when(pair + k < pairs)
                    def _():
                        total_copy(k, pair, h).start()

    conv_thirds = []
    small_copy(0).wait()
    norm(0)
    small_copy(1).wait()
    weight_wait(0)
    for n in range(2, 7):
        weight_copy(n).start()
    product = scan_product(0)
    if nb > 1:
        norm(1)
    for t in range(nb):
        if t + 2 < nb:
            arrive(t + 2)
        thirds = [n for n in range(3) if t == max(nb - 3 + min(n, 1), 0)]
        for n in thirds:
            weight_copy(2 + n).wait()
        if t + 1 < nb:
            later = scan_product(t + 1)
        for n in thirds:
            conv_thirds.append(conv_third(n))
        if t + 2 < nb:
            normalize(t + 2)
        if t == nb - 1:
            for n in (2, 3, 4):
                small_copy(n).wait()
            conv_block(0, jnp.concatenate(conv_thirds, axis=1))
        scan_block(t, product)
        product = later
    sent_state[:, :GROUP_FEATURES, :] = state[...].astype(bf16)
    for h in range(heads):
        put_decay(sent_state, h, jnp.exp(offset[0:1, head_slice(h)]))

    @pl.when(member == 0)
    def _():
        pl.semaphore_wait(twin_ready, 1)

    for h in range(heads):
        twin_copy(h).start()

    @pl.when(step > 0)
    def _():
        pl.semaphore_wait(mate_ready, 1)

    pass_own(CONV, True, (0, 1))

    if nb > 1:
        product = conv_product(1)
    for t in range(1, nb):
        if t + 1 < nb:
            later = conv_product(t + 1)
        conv_block(t, product)
        product = later

    weight_wait(2)

    def read_product(t):
        return dot(normed_all[block(t), :], w_read[...])

    def read_block(t, both):
        at = block(t)
        query = jax.nn.silu(both[:, :width].astype(bf16).astype(f32))
        outgate = jax.nn.silu(both[:, width:].astype(bf16).astype(f32))
        for h in range(heads):
            s = head_slice(h)
            gate[at, s] = outgate[:, s] * state_gain[...]
        for b in range(rows // CHUNK):
            lo, hi = b * CHUNK, (b + 1) * CHUNK
            where = pl.ds(t * rows + lo, CHUNK)
            number = t * (rows // CHUNK) + b
            cum = cums[where, :]
            mid = cum[CHUNK // 2 - 1 : CHUNK // 2]
            q_mid = query[lo:hi] * jnp.exp(cum - mid)
            q_all = q_mid * jnp.exp(mid)
            qdev[where, :] = (q_all * jnp.exp(offsets[number, 0:1, :])).astype(bf16)
            q_mid, q_all = q_mid.astype(bf16), q_all.astype(bf16)
            for h in range(heads):
                s = head_slice(h)
                scores = dot(q_mid[:, s], key_mid[where, s], ((1,), (1,)))
                scores = jnp.where(causal, scores, 0.0).astype(bf16)
                read[where, s] = dot(scores, value_all[where, s]) + dot(
                    q_all[:, s], olds[number, h], ((1,), (1,))
                )

        if t == nb // 2:
            pass_mates(CONV)

        @pl.when(t == nb - 1)
        def _():
            @pl.when(place == 0)
            def _():
                rim[...] = jnp.zeros_like(rim)

            @pl.when(place > 0)
            def _():
                rim_copy.wait_recv()

            ext = jnp.concatenate([rim[...], head_conv[...]], axis=0)
            w_taps = taps[...].astype(f32)
            fixed = w_taps[TAPS - 1 : TAPS] * head_conv[...]
            for j in range(TAPS - 1):
                lo = HALO - (TAPS - 1) + j
                fixed += w_taps[j : j + 1] * ext[lo : lo + HALO]
            fixed = per_group(head_gate[...] * fixed, group_gain[...])
            conv_all[me, 0:HALO, :] = fixed.astype(bf16)
            start(own_copies(CONV, nb))

            @pl.when(step > 0)
            def _():
                pass_own(MIX, False, (0,))
                pass_mates(MIX)


    product = read_product(0)
    for t in range(nb):
        if t + 1 < nb:
            later = read_product(t + 1)
        read_block(t, product)
        product = later

    for k in range(1, pairs):
        @pl.when(pair >= k)
        def _():
            for h in range(heads):
                total_copy(k, pair - k, h).wait_recv()
    incoming[...] = jnp.zeros_like(incoming)

    def hop(p, _):
        for h in range(heads):
            decay = decay_of(totals[p, h, GROUP_FEATURES:, :])
            incoming[h] = incoming[h] * decay + totals[p, h, :GROUP_FEATURES, :].astype(f32)
        return 0

    lax.fori_loop(0, pair, hop, 0)
    for h in range(heads):
        decay = decay_of(peer_state[h, GROUP_FEATURES:, :])
        through = incoming[h] * decay + peer_state[h, :GROUP_FEATURES, :].astype(f32)
        incoming[h] = jnp.where(member == 0, incoming[h], through)

    def merge(t, _):
        at = block(t)
        for h in range(heads):
            s = head_slice(h)
            whole = read[at, s] + dot(qdev[at, s], incoming[h].astype(bf16), ((1,), (1,)))
            mix_all[me, at, s] = (rms(whole) * gate[at, s]).astype(bf16)
        for n in range(rows // MIX_ROWS):
            start(own_copies(MIX, t * (rows // MIX_ROWS) + n))
        return 0

    lax.fori_loop(0, nb, merge, 0)

    mine_both, pair_both = columns.at[:, me], columns.at[:, partner]
    pltpu.make_async_copy(mine_both, mine_both, own_sem.at[0]).wait()
    pltpu.make_async_copy(pair_both, pair_both, pair_recv.at[0]).wait()

    def near(kind, t):
        out = dot(held[kind][me, block(t), :], columns[kind, me])
        return out + dot(held[kind][partner, block(t), :], columns[kind, partner])

    def near_conv(t, _):
        acc_all[block(t), :] = near(CONV, t)
        return 0

    first_landed(CONV)
    lax.fori_loop(0, nb, near_conv, 0)

    def near_mix(t, _):
        acc_all[block(t), :] += near(MIX, t)
        return 0

    first_landed(MIX)
    lax.fori_loop(0, nb, near_mix, 0)

    @pl.when(step < 0)
    def _():
        pass_mates(MIX)

    relay(CONV, 0)

    for kind in (CONV, MIX):
        for k, c in far_devices:
            piece_in(kind, k, c, 2).wait()
    for k in range(1, chips):
        landed(CONV, chips - 1 + k, 0)

    def far_conv(t, _):
        acc = acc_all[block(t), :]
        for k, c in far_devices:
            origin = far(k, c)
            acc += dot(conv_all[origin, block(t), :], columns[CONV, origin])
        acc_all[block(t), :] = acc
        return 0

    lax.fori_loop(0, nb, far_conv, 0)

    sent(CONV)
    passed_on(CONV)
    for kind in (CONV, MIX):
        for k, c in far_devices:
            piece_out(kind, k, c).wait_send()
            passed = columns.at[kind, me, 0 : 3 * piece]
            pltpu.make_async_copy(passed, passed, mate_send.at[kind, k - 1, c]).wait()
    pltpu.make_async_copy(mine_both, mine_both, pair_send.at[0]).wait()

    @pl.when(place < sp - 1)
    def _():
        rim_copy.wait_send()

    for h in range(heads):
        twin_copy(h).wait_send()
    for k in range(1, pairs):
        @pl.when(pair + k < pairs)
        def _():
            for h in range(heads):
                total_copy(k, pair, h).wait_send()

    def finish(t, _):
        @pl.when(t + LAG < mix_nb)
        def _():
            relay(MIX, t + LAG)

        for k in range(1, chips):
            landed(MIX, chips - 1 + k, t)
        at = mix_block(t)
        acc = acc_all[at, :]
        for k, c in far_devices:
            origin = far(k, c)
            acc += dot(mix_all[origin, at, :], columns[MIX, origin])
        result[at, :] = acc.astype(bf16)
        return 0

    for t in range(min(LAG, mix_nb)):
        relay(MIX, t)
    lax.fori_loop(0, mix_nb, finish, 0)

    sent(MIX)
    passed_on(MIX)


def body(
    tokens, in_gain, w_query, w_forget, w_input, w_outgate, w_conv_h, w_conv_b, w_conv_c,
    forget_floor, forget_leak, state_gain, conv_taps, group_gain, out_state, out_conv,
):
    count, feats = tokens.shape
    width, channels = w_query.shape[1], w_conv_h.shape[1]
    heads = width // GROUP_FEATURES
    tp, sp = lax.axis_size("tp"), lax.axis_size("sp")
    ncols, nb, chips = out_state.shape[1] // tp, count // ROWS, tp // 2
    share = min(SHARE, sp)
    chunks, pairs = count // CHUNK, sp // 2

    hbm = pl.BlockSpec(memory_space=pltpu.HBM)
    vmem = pl.BlockSpec(memory_space=pltpu.VMEM)
    sems = pltpu.SemaphoreType.DMA
    square = (heads, GROUP_FEATURES, GROUP_FEATURES)
    longer = (heads, GROUP_FEATURES + EXTRA, GROUP_FEATURES)
    return pl.pallas_call(
        functools.partial(fused_kernel, tp, sp, share),
        in_specs=[hbm] * 16,
        out_specs=vmem,
        out_shape=pltpu.VMEM((count, ncols), bf16),
        scratch_shapes=[
            pltpu.VMEM((1, feats), f32),
            pltpu.VMEM((1, width), f32),
            pltpu.VMEM((1, GROUP_FEATURES), f32),
            pltpu.VMEM((TAPS, channels), bf16),
            pltpu.VMEM((1, GROUP_FEATURES), f32),
            sems((5,)),
            pltpu.VMEM((count, feats), bf16),
            pltpu.VMEM((feats, 2 * width), bf16),
            pltpu.VMEM((feats, 3 * channels), bf16),
            pltpu.VMEM((feats, 2 * width), bf16),
            pltpu.VMEM((count, width), f32),
            pltpu.VMEM((count, width), bf16),
            pltpu.VMEM((count, width), bf16),
            pltpu.VMEM((chunks,) + square, bf16),
            pltpu.VMEM((chunks, HALO, width), f32),
            pltpu.VMEM((HALO + ROWS, channels), f32),
            pltpu.VMEM(square, f32),
            pltpu.VMEM((HALO, width), f32),
            pltpu.VMEM((count, width), f32),
            pltpu.VMEM((count, width), bf16),
            pltpu.VMEM((count, width), f32),
            pltpu.VMEM((tp, count, channels), bf16),
            pltpu.VMEM((tp, count, width), bf16),
            pltpu.VMEM((2, tp, width, ncols), bf16),
            pltpu.VMEM((count, ncols), f32),
            pltpu.VMEM(longer, bf16),
            pltpu.VMEM(longer, bf16),
            pltpu.VMEM(longer, bf16),
            pltpu.VMEM((pairs,) + longer, bf16),
            pltpu.VMEM((HALO, channels), f32),
            pltpu.VMEM((HALO, channels), f32),
            pltpu.VMEM((HALO, channels), f32),
            pltpu.VMEM((HALO, channels), f32),
            pltpu.VMEM(square, f32),
            sems((nb,)), sems((2,)), sems((5,)), sems((1,)),
            sems((1,)), sems((1,)), sems((2, chips - 1, 2)), sems((2, chips - 1, 2, 3)),
            sems((2, chips - 1, 2)),
            sems((2, chips)), sems((2, chips - 1)), sems((2 * chips - 1,)), sems((1,)),
            sems((2 * chips - 2, count // MIX_ROWS)),
            sems((heads,)), sems((heads,)), sems((heads, pairs - 1)), sems((heads, pairs)),
            sems((1,)), sems((1,)),
        ] + [pltpu.SemaphoreType.REGULAR] * 4,
        compiler_params=pltpu.CompilerParams(
            vmem_limit_bytes=56 * 2**20, collective_id=0, has_side_effects=True
        ),
    )(
        tokens, in_gain[None], w_query, w_forget, w_input, w_outgate, w_conv_h, w_conv_b, w_conv_c,
        forget_floor[None], forget_leak, state_gain[None], conv_taps, group_gain[None],
        out_state, out_conv,
    )


def solution(mesh):
    cols, rows = P(None, "tp"), P("tp", None)
    in_specs = (
        P("sp", None), P(), cols, cols, cols, cols, cols, cols, cols,
        P("tp"), P("sp", "tp"), P(), cols, P(), rows, rows,
    )
    return jax.shard_map(
        body, mesh=mesh, in_specs=in_specs, out_specs=P("sp", "tp"), check_vma=False
    )
```

```python
import functools

import jax
import jax.numpy as jnp
from jax import lax
from jax.experimental import pallas as pl
from jax.experimental.pallas import tpu as pltpu
from jax.sharding import PartitionSpec as P

GROUP_FEATURES = 128
CHUNK = 128
ROWS = 256
MIX_ROWS = 128
LAG = 2
EXTRA = 8
TAPS = 3
HALO = 8
HEAD = 16
SHARE = 4
CONV, MIX = 0, 1

norm_eps = 1e-06
f32 = jnp.float32
bf16 = jnp.bfloat16


def dot(a, b, dims=((1,), (0,))):
    return lax.dot_general(a, b, (dims, ((), ())), preferred_element_type=f32)


def rms(values):
    return values * lax.rsqrt(jnp.mean(values * values, axis=-1, keepdims=True) + norm_eps)


def per_group(values, gain):
    parts = []
    for g in range(values.shape[1] // GROUP_FEATURES):
        parts.append(rms(values[:, g * GROUP_FEATURES : (g + 1) * GROUP_FEATURES]) * gain)
    return jnp.concatenate(parts, axis=1)


def head_slice(h):
    return slice(h * GROUP_FEATURES, (h + 1) * GROUP_FEATURES)


def prefix_sum(ones, values):
    high = values.astype(bf16)
    rest = values - high.astype(f32)
    middle = rest.astype(bf16)
    low = (rest - middle.astype(f32)).astype(bf16)
    return dot(ones, jnp.concatenate([high, middle, low], axis=0))


def fused_kernel(
    tp, sp, share,
    tokens, in_gain_in, wq, wf, wi, wg, wh, wb, wc, floor_in, leak, state_gain_in, taps_in,
    group_gain_in, out_state, out_conv, result,
    in_gain, floor, state_gain, taps, group_gain, small_sem,
    normed_all, w_scan, w_conv, w_read, cums, key_mid, value_all, olds, offsets,
    pad, state, offset, read, qdev, gate, conv_all, mix_all, columns, acc_all,
    sent_state, peer_state, sent_total, totals,
    rim, tail, head_conv, head_gate, incoming,
    tok_sem, leak_sem, w_sem, own_sem,
    pair_send, pair_recv, piece_send, piece_recv, twin_recv, mate_send,
    blk_send, fwd_send, conv_recv, mix_first, mix_recv, l1_send, l1_recv, l2_send, l2_recv, rim_send, rim_recv,
    ready, rim_ready, twin_ready, mate_ready,
):
    me, place = lax.axis_index("tp"), lax.axis_index("sp")
    partner = me + 1 - 2 * lax.rem(me, 2)
    chips = tp // 2
    chip = lax.div(me, 2)
    core = lax.rem(me, 2)
    count, feats = normed_all.shape
    width = value_all.shape[1]
    channels = pad.shape[1]
    rows = ROWS
    nb, mix_nb = count // rows, count // MIX_ROWS
    ncols = result.shape[1]
    heads = state.shape[0]
    piece = width // share
    mine = lax.rem(place, share)
    twin = place + 1 - 2 * lax.rem(place, 2)
    across = share // 2
    step = across - share * lax.div(mine, across)
    mate, mates_piece = place + step, mine + step
    member = lax.rem(place, 2)
    pair = lax.div(place, 2)
    pairs = sp // 2
    before, after = lax.rem(place + sp - 1, sp), lax.rem(place + 1, sp)
    held = (conv_all, mix_all)
    outs = (out_conv, out_state)

    def block(t):
        if isinstance(t, int):
            return pl.ds(t * rows, rows)
        return pl.ds(pl.multiple_of(t * rows, rows), rows)

    def mix_block(t):
        return pl.ds(pl.multiple_of(t * MIX_ROWS, MIX_ROWS), MIX_ROWS)

    def token_copy(t):
        return pltpu.make_async_copy(tokens.at[block(t)], normed_all.at[block(t)], tok_sem.at[t])

    def leak_copy(t):
        at = block(0) if t == 0 else pl.ds(rows, count - rows)
        return pltpu.make_async_copy(leak.at[at], cums.at[at], leak_sem.at[t])

    weights = ((wf, 0, 0), (wi, 0, 1), (wc, 1, 0), (wh, 1, 1), (wb, 1, 2), (wq, 2, 0), (wg, 2, 1))
    weight_sems = (0, 0, 1, 2, 3, 4, 4)

    phases = [w_scan, w_conv, w_read]

    def weight_copy(n):
        src, phase, slot = weights[n]
        dst = phases[phase]
        return pltpu.make_async_copy(
            src, dst.at[:, slot * width : (slot + 1) * width], w_sem.at[weight_sems[n]]
        )

    def weight_wait(phase):
        dst = phases[phase]
        pltpu.make_async_copy(dst, dst, w_sem.at[weight_sems[2 * phase + phase // 2]]).wait()

    def cols_of(device):
        return pl.ds(pl.multiple_of(device * ncols, ncols), ncols)

    def piece_rows(g):
        return pl.ds(pl.multiple_of(g * piece, piece), piece)

    def own_columns(kind):
        return pltpu.make_async_copy(
            outs[kind].at[:, cols_of(me)], columns.at[kind, me], own_sem.at[0]
        )

    def pair_columns(kind, origin):
        return pltpu.make_async_remote_copy(
            outs[kind].at[:, cols_of(partner)], columns.at[kind, origin],
            pair_send.at[0], pair_recv.at[0], device_id={"tp": partner},
        )

    def far(k, c):
        return lax.rem(chip + k, chips) * 2 + c

    def piece_out(kind, k, c):
        target = far(k, c)
        return pltpu.make_async_remote_copy(
            outs[kind].at[piece_rows(mine), cols_of(target)],
            columns.at[kind, me, piece_rows(mine)],
            piece_send.at[0], piece_recv.at[kind, chips - k - 1, core, 0],
            device_id={"tp": target},
        )

    def piece_in(kind, k, c, n):
        ref = columns.at[kind, me, 0:piece]
        return pltpu.make_async_copy(ref, ref, piece_recv.at[kind, k - 1, c, n])

    def pass_on(kind, k, c, n):
        g, to = ((mine, mate), (mine, twin), (mates_piece, twin))[n]
        ref = columns.at[kind, far(k, c), piece_rows(g)]
        return pltpu.make_async_remote_copy(
            ref, ref, mate_send.at[0],
            piece_recv.at[kind, k - 1, c, 1] if n == 0 else twin_recv.at[0],
            device_id={"sp": to},
        )

    def pieces_wait(n, sem):
        ref = columns.at[:, 0 : tp - 2, 0 : n * piece]
        pltpu.make_async_copy(ref, ref, sem.at[0]).wait()

    def pass_own(kind, wait, which):
        for k, c in far_devices:
            if wait:
                piece_in(kind, k, c, 0).wait()
            for n in which:
                pass_on(kind, k, c, n).start()

    def pass_mates(kind):
        for k, c in far_devices:
            piece_in(kind, k, c, 1).wait()
            pass_on(kind, k, c, 2).start()

    far_devices = [(k, c) for k in range(1, chips) for c in range(2)]

    def span(kind, t):
        if kind == CONV and isinstance(t, int):
            if t == 0:
                return pl.ds(HEAD, rows - HEAD)
            if t == nb:
                return pl.ds(0, HEAD)
        return mix_block(t) if kind == MIX else block(t)

    def recv_sem(kind, slot, t):
        return conv_recv.at[slot] if kind == CONV or slot == 0 else mix_recv.at[slot - 1, t]

    def first_recv(kind):
        return (conv_recv if kind == CONV else mix_first).at[0]

    def own_copies(kind, t):
        ref = held[kind].at[me, span(kind, t)]
        out = []
        for k in range(1, chips):
            out.append(pltpu.make_async_remote_copy(
                ref, ref, blk_send.at[kind, k], recv_sem(kind, chips - k, t),
                device_id={"tp": far(k, core)},
            ))
        out.append(pltpu.make_async_remote_copy(
            ref, ref, blk_send.at[kind, 0], first_recv(kind), device_id={"tp": partner}
        ))
        return out

    def relays(kind, t):
        out = []
        for k in range(1, chips):
            ref = held[kind].at[far(k, core)]
            if kind == MIX:
                ref = ref.at[mix_block(t)]
            out.append(pltpu.make_async_remote_copy(
                ref, ref, fwd_send.at[kind, k - 1], recv_sem(kind, chips - 1 + k, t),
                device_id={"tp": partner},
            ))
        return out

    def start(copies):
        for copy in copies:
            copy.start()

    def landed(kind, slot, t):
        ref = held[kind].at[me]
        if kind == MIX:
            ref = ref.at[mix_block(t)]
        pltpu.make_async_copy(ref, ref, recv_sem(kind, slot, t)).wait()

    def relay(kind, t):
        for k, copy in enumerate(relays(kind, t)):
            landed(kind, k + 1, t)
            copy.start()

    def first_landed(kind):
        ref = held[kind].at[me]
        pltpu.make_async_copy(ref, ref, first_recv(kind)).wait()

    def sent(kind):
        ref = held[kind].at[me]
        for k in range(chips):
            pltpu.make_async_copy(ref, ref, blk_send.at[kind, k]).wait()

    def passed_on(kind):
        ref = held[kind].at[me]
        for k in range(1, chips):
            pltpu.make_async_copy(ref, ref, fwd_send.at[kind, k - 1]).wait()

    def twin_copy(h):
        return pltpu.make_async_remote_copy(
            sent_state.at[h], peer_state.at[h], l1_send.at[0], l1_recv.at[h],
            device_id={"sp": twin},
        )

    def total_copy(k, source, h):
        return pltpu.make_async_remote_copy(
            sent_total.at[h], totals.at[source, h], l2_send.at[k - 1], l2_recv.at[source],
            device_id={"sp": lax.rem(place + 2 * k, sp)},
        )

    def put_decay(ref, h, decay):
        high = decay.astype(bf16)
        low = (decay - high.astype(f32)).astype(bf16)
        both = jnp.concatenate([high, low], axis=0)
        ref[h, GROUP_FEATURES:, :] = jnp.concatenate([both] * (EXTRA // 2), axis=0)

    def decay_of(rows_of):
        both = rows_of.astype(f32)
        return both[0:1] + both[1:2]

    rim_copy = pltpu.make_async_remote_copy(
        tail, rim, rim_send.at[0], rim_recv.at[0], device_id={"sp": after}
    )

    small = ((in_gain_in, in_gain), (floor_in, floor), (state_gain_in, state_gain),
             (taps_in, taps), (group_gain_in, group_gain))

    def small_copy(n):
        return pltpu.make_async_copy(small[n][0], small[n][1], small_sem.at[n])

    small_copy(0).start()
    token_copy(0).start()
    weight_copy(0).start()
    weight_copy(1).start()
    small_copy(1).start()
    leak_copy(0).start()
    if nb > 1:
        token_copy(1).start()
        leak_copy(1).start()
    barrier = pltpu.get_barrier_semaphore()
    for k in range(1, tp):
        pl.semaphore_signal(barrier, inc=1, device_id={"tp": lax.rem(me + k, tp)})
    for to, low in ((twin, member == 0), (mate, step > 0)):
        @pl.when(low)
        def _():
            pl.semaphore_signal(barrier, inc=1, device_id={"sp": to})

    for k in range(1, pairs):
        @pl.when(pair + k < pairs)
        def _():
            pl.semaphore_signal(barrier, inc=1, device_id={"sp": lax.rem(place + 2 * k, sp)})
    follows = jnp.logical_and(member == 0, pair > 0)
    leads = jnp.logical_and(member == 1, pair < pairs - 1)

    @pl.when(leads)
    def _():
        pl.semaphore_signal(barrier, inc=1, device_id={"sp": after})

    lower = pair + member + jnp.where(step > 0, 0, 1) + jnp.where(follows, 1, 0)
    pl.semaphore_wait(barrier, tp - 1 + lower)

    @pl.when(member == 1)
    def _():
        pl.semaphore_signal(twin_ready, inc=1, device_id={"sp": twin})

    @pl.when(step < 0)
    def _():
        pl.semaphore_signal(mate_ready, inc=1, device_id={"sp": mate})

    for k in range(1, pairs):
        @pl.when(pair >= k)
        def _():
            pl.semaphore_signal(ready, inc=1, device_id={"sp": lax.rem(place + sp - 2 * k, sp)})

    @pl.when(follows)
    def _():
        pl.semaphore_signal(rim_ready, inc=1, device_id={"sp": before})
    for kind in (CONV, MIX):
        for k, c in far_devices:
            piece_out(kind, k, c).start()
    for t in range(2, nb):
        token_copy(t).start()
    for n in (2, 3, 4):
        weight_copy(n).start()
    for n in (2, 3, 4):
        small_copy(n).start()
    for kind in (CONV, MIX):
        pair_columns(kind, me).start()
        own_columns(kind).start()

    state[...] = jnp.zeros_like(state)
    offset[...] = jnp.zeros_like(offset)
    pad[0:HALO, :] = jnp.zeros((HALO, channels), f32)

    r = lax.broadcasted_iota(jnp.int32, (CHUNK, CHUNK), 0)
    c = lax.broadcasted_iota(jnp.int32, (CHUNK, CHUNK), 1)
    causal = r >= c
    ones = jnp.concatenate([causal.astype(f32)] * 3, axis=1).astype(bf16)

    def arrive(t):
        token_copy(t).wait()
        if t < 2:
            leak_copy(t).wait()

    def norm(t):
        arrive(t)
        normalize(t)

    def normalize(t):
        at = block(t)
        normed_all[at, :] = (rms(normed_all[at, :].astype(f32)) * in_gain[...]).astype(bf16)

    def scan_product(t):
        return dot(normed_all[block(t), :], w_scan[...])

    def scan_block(t, both):
        at = block(t)
        x = both[:, :width].astype(bf16).astype(f32)
        value = both[:, width:].astype(bf16)
        value_all[at, :] = value
        key = (1.0 - floor[...]) * jax.nn.sigmoid(-x)
        logf = jnp.log(1.0 - key) + cums[at, :]
        for b in range(rows // CHUNK):
            lo, hi = b * CHUNK, (b + 1) * CHUNK
            where = pl.ds(t * rows + lo, CHUNK)
            number = t * (rows // CHUNK) + b
            cum = prefix_sum(ones, logf[lo:hi])
            mid = cum[CHUNK // 2 - 1 : CHUNK // 2]
            last = cum[CHUNK - 1 : CHUNK]
            k_mid = key[lo:hi] * jnp.exp(mid - cum)
            k_end = (k_mid * jnp.exp(last - mid)).astype(bf16)
            cums[where, :] = cum
            key_mid[where, :] = k_mid.astype(bf16)
            offsets[number] = offset[...]
            for h in range(heads):
                s = head_slice(h)
                old = state[h]
                olds[number, h] = old.astype(bf16)
                state[h] = old * jnp.exp(last[:, s]) + dot(
                    value[lo:hi, s], k_end[:, s], ((0,), (0,))
                )
            offset[...] += last

    def conv_third(n):
        return dot(normed_all[block(0), :], w_conv[:, n * channels : (n + 1) * channels])


    def conv_product(t):
        return dot(normed_all[block(t), :], w_conv[...])

    def conv_block(t, three):
        at = block(t)
        first = three[:, :channels].astype(bf16).astype(f32)
        second = three[:, channels : 2 * channels].astype(bf16).astype(f32)
        proj_b = three[:, 2 * channels :].astype(bf16).astype(f32)
        conv_in = (first * second).astype(bf16).astype(f32)
        w_taps = taps[...].astype(f32)
        pad[HALO : HALO + rows, :] = conv_in
        total = w_taps[TAPS - 1 : TAPS] * conv_in
        for j in range(TAPS - 1):
            lo = HALO - (TAPS - 1) + j
            total += w_taps[j : j + 1] * pad[lo : lo + rows, :]
        conv_all[me, at, :] = per_group(proj_b * total, group_gain[...]).astype(bf16)

        @pl.when(t == 0)
        def _():
            head_conv[...] = conv_in[:HALO]
            head_gate[...] = proj_b[:HALO]
            start(own_copies(CONV, 0))

        @pl.when(t > 0)
        def _():
            start(own_copies(CONV, t))

        pad[0:HALO, :] = conv_in[rows - HALO :]

        @pl.when(t == nb - 1)
        def _():
            tail[...] = conv_in[rows - HALO :]

            @pl.when(leads)
            def _():
                pl.semaphore_wait(rim_ready, 1)

            @pl.when(place < sp - 1)
            def _():
                rim_copy.start()

            pass_own(MIX, True, (1,))

            @pl.when(step < 0)
            def _():
                pass_own(MIX, False, (0,))


        @pl.when(t == nb - 1)
        def _():
            @pl.when(pair < pairs - 1)
            def _():
                pl.semaphore_wait(ready, pairs - 1 - pair)

            for h in range(heads):
                s = head_slice(h)
                twin_copy(h).wait_recv()
                own, other = state[h], peer_state[h, :GROUP_FEATURES, :].astype(f32)
                own_decay = jnp.exp(offset[0:1, s])
                peer_decay = decay_of(peer_state[h, GROUP_FEATURES:, :])
                early = jnp.where(member == 0, own, other)
                late = jnp.where(member == 0, other, own)
                decay = jnp.where(member == 0, peer_decay, own_decay)
                sent_total[h, :GROUP_FEATURES, :] = (early * decay + late).astype(bf16)
                put_decay(sent_total, h, own_decay * peer_decay)
                for k in reversed(range(1, pairs)):
                    @pl.when(pair + k < pairs)
                    def _():
                        total_copy(k, pair, h).start()

    conv_thirds = []
    small_copy(0).wait()
    norm(0)
    small_copy(1).wait()
    weight_wait(0)
    for n in (5, 6):
        weight_copy(n).start()
    product = scan_product(0)
    if nb > 1:
        norm(1)
    for t in range(nb):
        if t + 2 < nb:
            arrive(t + 2)
        thirds = [n for n in range(3) if t == max(nb - 4 + min(n, 1), 0)]
        for n in thirds:
            weight_copy(2 + n).wait()
        if t + 1 < nb:
            later = scan_product(t + 1)
        for n in thirds:
            conv_thirds.append(conv_third(n))
        if t + 2 < nb:
            normalize(t + 2)
        if t == max(nb - 2, 0):
            for n in (2, 3, 4):
                small_copy(n).wait()
            conv_block(0, jnp.concatenate(conv_thirds, axis=1))
        scan_block(t, product)
        product = later
    sent_state[:, :GROUP_FEATURES, :] = state[...].astype(bf16)
    for h in range(heads):
        put_decay(sent_state, h, jnp.exp(offset[0:1, head_slice(h)]))

    @pl.when(member == 0)
    def _():
        pl.semaphore_wait(twin_ready, 1)

    for h in range(heads):
        twin_copy(h).start()

    @pl.when(step > 0)
    def _():
        pl.semaphore_wait(mate_ready, 1)

    pass_own(CONV, True, (0, 1))

    if nb > 1:
        product = conv_product(1)
    for t in range(1, nb):
        if t + 1 < nb:
            later = conv_product(t + 1)
        conv_block(t, product)
        product = later

    weight_wait(2)

    def read_product(t):
        return dot(normed_all[block(t), :], w_read[...])

    def read_block(t, both):
        at = block(t)
        query = jax.nn.silu(both[:, :width].astype(bf16).astype(f32))
        outgate = jax.nn.silu(both[:, width:].astype(bf16).astype(f32))
        for h in range(heads):
            s = head_slice(h)
            gate[at, s] = outgate[:, s] * state_gain[...]
        for b in range(rows // CHUNK):
            lo, hi = b * CHUNK, (b + 1) * CHUNK
            where = pl.ds(t * rows + lo, CHUNK)
            number = t * (rows // CHUNK) + b
            cum = cums[where, :]
            mid = cum[CHUNK // 2 - 1 : CHUNK // 2]
            q_mid = query[lo:hi] * jnp.exp(cum - mid)
            q_all = q_mid * jnp.exp(mid)
            qdev[where, :] = (q_all * jnp.exp(offsets[number, 0:1, :])).astype(bf16)
            q_mid, q_all = q_mid.astype(bf16), q_all.astype(bf16)
            for h in range(heads):
                s = head_slice(h)
                scores = dot(q_mid[:, s], key_mid[where, s], ((1,), (1,)))
                scores = jnp.where(causal, scores, 0.0).astype(bf16)
                read[where, s] = dot(scores, value_all[where, s]) + dot(
                    q_all[:, s], olds[number, h], ((1,), (1,))
                )

        if t == nb // 2:
            pass_mates(CONV)

        @pl.when(t == nb - 1)
        def _():
            @pl.when(place == 0)
            def _():
                rim[...] = jnp.zeros_like(rim)

            @pl.when(place > 0)
            def _():
                rim_copy.wait_recv()

            ext = jnp.concatenate([rim[...], head_conv[...]], axis=0)
            w_taps = taps[...].astype(f32)
            fixed = w_taps[TAPS - 1 : TAPS] * head_conv[...]
            for j in range(TAPS - 1):
                lo = HALO - (TAPS - 1) + j
                fixed += w_taps[j : j + 1] * ext[lo : lo + HALO]
            fixed = per_group(head_gate[...] * fixed, group_gain[...])
            conv_all[me, 0:HALO, :] = fixed.astype(bf16)
            start(own_copies(CONV, nb))

            @pl.when(step > 0)
            def _():
                pass_own(MIX, False, (0,))
                pass_mates(MIX)


    product = read_product(0)
    for t in range(nb):
        if t + 1 < nb:
            later = read_product(t + 1)
        read_block(t, product)
        product = later

    for k in range(1, pairs):
        @pl.when(pair >= k)
        def _():
            ref = totals.at[pair - k]
            pltpu.make_async_copy(ref, ref, l2_recv.at[pair - k]).wait()
    incoming[...] = jnp.zeros_like(incoming)

    def hop(p, _):
        for h in range(heads):
            decay = decay_of(totals[p, h, GROUP_FEATURES:, :])
            incoming[h] = incoming[h] * decay + totals[p, h, :GROUP_FEATURES, :].astype(f32)
        return 0

    lax.fori_loop(0, pair, hop, 0)
    for h in range(heads):
        decay = decay_of(peer_state[h, GROUP_FEATURES:, :])
        through = incoming[h] * decay + peer_state[h, :GROUP_FEATURES, :].astype(f32)
        incoming[h] = jnp.where(member == 0, incoming[h], through)

    def merge(t, _):
        at = block(t)
        for h in range(heads):
            s = head_slice(h)
            whole = read[at, s] + dot(qdev[at, s], incoming[h].astype(bf16), ((1,), (1,)))
            mix_all[me, at, s] = (rms(whole) * gate[at, s]).astype(bf16)
        for n in range(rows // MIX_ROWS):
            start(own_copies(MIX, t * (rows // MIX_ROWS) + n))
        return 0

    lax.fori_loop(0, nb, merge, 0)

    mine_both, pair_both = columns.at[:, me], columns.at[:, partner]
    pltpu.make_async_copy(mine_both, mine_both, own_sem.at[0]).wait()
    pltpu.make_async_copy(pair_both, pair_both, pair_recv.at[0]).wait()

    def near(kind, t):
        out = dot(held[kind][me, block(t), :], columns[kind, me])
        return out + dot(held[kind][partner, block(t), :], columns[kind, partner])

    def near_conv(t, _):
        acc_all[block(t), :] = near(CONV, t)
        return 0

    first_landed(CONV)
    lax.fori_loop(0, nb, near_conv, 0)

    def near_mix(t, _):
        acc_all[block(t), :] += near(MIX, t)
        return 0

    first_landed(MIX)
    lax.fori_loop(0, nb, near_mix, 0)

    @pl.when(step < 0)
    def _():
        pass_mates(MIX)

    relay(CONV, 0)

    pieces_wait(2, twin_recv)
    for k in range(1, chips):
        landed(CONV, chips - 1 + k, 0)

    def far_conv(t, _):
        acc = acc_all[block(t), :]
        for k, c in far_devices:
            origin = far(k, c)
            acc += dot(conv_all[origin, block(t), :], columns[CONV, origin])
        acc_all[block(t), :] = acc
        return 0

    lax.fori_loop(0, nb, far_conv, 0)

    sent(CONV)
    passed_on(CONV)
    pieces_wait(1, piece_send)
    pieces_wait(3, mate_send)
    pltpu.make_async_copy(mine_both, mine_both, pair_send.at[0]).wait()

    @pl.when(place < sp - 1)
    def _():
        rim_copy.wait_send()

    pltpu.make_async_copy(sent_state, sent_state, l1_send.at[0]).wait()
    for k in range(1, pairs):
        @pl.when(pair + k < pairs)
        def _():
            pltpu.make_async_copy(sent_total, sent_total, l2_send.at[k - 1]).wait()

    def finish(t, _):
        @pl.when(t + LAG < mix_nb)
        def _():
            relay(MIX, t + LAG)

        for k in range(1, chips):
            landed(MIX, chips - 1 + k, t)
        at = mix_block(t)
        acc = acc_all[at, :]
        for k, c in far_devices:
            origin = far(k, c)
            acc += dot(mix_all[origin, at, :], columns[MIX, origin])
        result[at, :] = acc.astype(bf16)
        return 0

    for t in range(min(LAG, mix_nb)):
        relay(MIX, t)
    lax.fori_loop(0, mix_nb, finish, 0)

    sent(MIX)
    passed_on(MIX)


def body(
    tokens, in_gain, w_query, w_forget, w_input, w_outgate, w_conv_h, w_conv_b, w_conv_c,
    forget_floor, forget_leak, state_gain, conv_taps, group_gain, out_state, out_conv,
):
    count, feats = tokens.shape
    width, channels = w_query.shape[1], w_conv_h.shape[1]
    heads = width // GROUP_FEATURES
    tp, sp = lax.axis_size("tp"), lax.axis_size("sp")
    ncols, nb, chips = out_state.shape[1] // tp, count // ROWS, tp // 2
    share = min(SHARE, sp)
    chunks, pairs = count // CHUNK, sp // 2

    hbm = pl.BlockSpec(memory_space=pltpu.HBM)
    vmem = pl.BlockSpec(memory_space=pltpu.VMEM)
    sems = pltpu.SemaphoreType.DMA
    square = (heads, GROUP_FEATURES, GROUP_FEATURES)
    longer = (heads, GROUP_FEATURES + EXTRA, GROUP_FEATURES)
    return pl.pallas_call(
        functools.partial(fused_kernel, tp, sp, share),
        in_specs=[hbm] * 16,
        out_specs=vmem,
        out_shape=pltpu.VMEM((count, ncols), bf16),
        scratch_shapes=[
            pltpu.VMEM((1, feats), f32),
            pltpu.VMEM((1, width), f32),
            pltpu.VMEM((1, GROUP_FEATURES), f32),
            pltpu.VMEM((TAPS, channels), bf16),
            pltpu.VMEM((1, GROUP_FEATURES), f32),
            sems((5,)),
            pltpu.VMEM((count, feats), bf16),
            pltpu.VMEM((feats, 2 * width), bf16),
            pltpu.VMEM((feats, 3 * channels), bf16),
            pltpu.VMEM((feats, 2 * width), bf16),
            pltpu.VMEM((count, width), f32),
            pltpu.VMEM((count, width), bf16),
            pltpu.VMEM((count, width), bf16),
            pltpu.VMEM((chunks,) + square, bf16),
            pltpu.VMEM((chunks, HALO, width), f32),
            pltpu.VMEM((HALO + ROWS, channels), f32),
            pltpu.VMEM(square, f32),
            pltpu.VMEM((HALO, width), f32),
            pltpu.VMEM((count, width), f32),
            pltpu.VMEM((count, width), bf16),
            pltpu.VMEM((count, width), f32),
            pltpu.VMEM((tp, count, channels), bf16),
            pltpu.VMEM((tp, count, width), bf16),
            pltpu.VMEM((2, tp, width, ncols), bf16),
            pltpu.VMEM((count, ncols), f32),
            pltpu.VMEM(longer, bf16),
            pltpu.VMEM(longer, bf16),
            pltpu.VMEM(longer, bf16),
            pltpu.VMEM((pairs,) + longer, bf16),
            pltpu.VMEM((HALO, channels), f32),
            pltpu.VMEM((HALO, channels), f32),
            pltpu.VMEM((HALO, channels), f32),
            pltpu.VMEM((HALO, channels), f32),
            pltpu.VMEM(square, f32),
            sems((nb,)), sems((2,)), sems((5,)), sems((1,)),
            sems((1,)), sems((1,)), sems((1,)), sems((2, chips - 1, 2, 2)), sems((1,)), sems((1,)),
            sems((2, chips)), sems((2, chips - 1)), sems((2 * chips - 1,)), sems((1,)),
            sems((2 * chips - 2, count // MIX_ROWS)),
            sems((1,)), sems((heads,)), sems((pairs - 1,)), sems((pairs - 1,)),
            sems((1,)), sems((1,)),
        ] + [pltpu.SemaphoreType.REGULAR] * 4,
        compiler_params=pltpu.CompilerParams(
            vmem_limit_bytes=56 * 2**20, collective_id=0, has_side_effects=True
        ),
    )(
        tokens, in_gain[None], w_query, w_forget, w_input, w_outgate, w_conv_h, w_conv_b, w_conv_c,
        forget_floor[None], forget_leak, state_gain[None], conv_taps, group_gain[None],
        out_state, out_conv,
    )


def solution(mesh):
    cols, rows = P(None, "tp"), P("tp", None)
    in_specs = (
        P("sp", None), P(), cols, cols, cols, cols, cols, cols, cols,
        P("tp"), P("sp", "tp"), P(), cols, P(), rows, rows,
    )
    return jax.shard_map(
        body, mesh=mesh, in_specs=in_specs, out_specs=P("sp", "tp"), check_vma=False
    )
```

```python
import functools

import jax
import jax.numpy as jnp
from jax import lax
from jax.experimental import pallas as pl
from jax.experimental.pallas import tpu as pltpu
from jax.sharding import PartitionSpec as P

GROUP_FEATURES = 128
CHUNK = 128
ROWS = 256
MIX_ROWS = 128
LAG = 3
EXTRA = 8
TAPS = 3
HALO = 8
HEAD = 16
SHARE = 4
CONV, MIX = 0, 1

norm_eps = 1e-06
f32 = jnp.float32
bf16 = jnp.bfloat16


def dot(a, b, dims=((1,), (0,))):
    return lax.dot_general(a, b, (dims, ((), ())), preferred_element_type=f32)


def rms(values):
    return values * lax.rsqrt(jnp.mean(values * values, axis=-1, keepdims=True) + norm_eps)


def per_group(values, gain):
    parts = []
    for g in range(values.shape[1] // GROUP_FEATURES):
        parts.append(rms(values[:, g * GROUP_FEATURES : (g + 1) * GROUP_FEATURES]) * gain)
    return jnp.concatenate(parts, axis=1)


def head_slice(h):
    return slice(h * GROUP_FEATURES, (h + 1) * GROUP_FEATURES)


def prefix_sum(ones, values):
    high = values.astype(bf16)
    rest = values - high.astype(f32)
    middle = rest.astype(bf16)
    low = (rest - middle.astype(f32)).astype(bf16)
    return dot(ones, jnp.concatenate([high, middle, low], axis=0))


def fused_kernel(
    tp, sp, share,
    tokens, in_gain_in, wq, wf, wi, wg, wh, wb, wc, floor_in, leak, state_gain_in, taps_in,
    group_gain_in, out_state, out_conv, result,
    in_gain, floor, state_gain, taps, group_gain, small_sem,
    normed_all, w_scan, w_conv, w_read, cums, key_mid, value_all, olds, offsets,
    pad, state, offset, read, qdev, gate, conv_all, mix_all, columns, acc_all,
    sent_state, peer_state, sent_total, totals,
    rim, tail, head_conv, head_gate, incoming,
    tok_sem, leak_sem, w_sem, own_sem,
    pair_send, pair_recv, piece_send, piece_recv, twin_recv, mate_send,
    blk_send, fwd_send, conv_recv, mix_first, mix_recv, l1_send, l1_recv, l2_send, l2_recv, rim_send, rim_recv,
    ready, rim_ready, twin_ready, mate_ready,
):
    me, place = lax.axis_index("tp"), lax.axis_index("sp")
    partner = me + 1 - 2 * lax.rem(me, 2)
    chips = tp // 2
    chip = lax.div(me, 2)
    core = lax.rem(me, 2)
    count, feats = normed_all.shape
    width = value_all.shape[1]
    channels = pad.shape[1]
    rows = ROWS
    nb, mix_nb = count // rows, count // MIX_ROWS
    ncols = result.shape[1]
    heads = state.shape[0]
    piece = width // share
    mine = lax.rem(place, share)
    twin = place + 1 - 2 * lax.rem(place, 2)
    across = share // 2
    step = across - share * lax.div(mine, across)
    mate, mates_piece = place + step, mine + step
    member = lax.rem(place, 2)
    pair = lax.div(place, 2)
    pairs = sp // 2
    before, after = lax.rem(place + sp - 1, sp), lax.rem(place + 1, sp)
    held = (conv_all, mix_all)
    outs = (out_conv, out_state)

    def block(t):
        if isinstance(t, int):
            return pl.ds(t * rows, rows)
        return pl.ds(pl.multiple_of(t * rows, rows), rows)

    def mix_block(t):
        return pl.ds(pl.multiple_of(t * MIX_ROWS, MIX_ROWS), MIX_ROWS)

    def token_copy(t):
        return pltpu.make_async_copy(tokens.at[block(t)], normed_all.at[block(t)], tok_sem.at[t])

    def leak_copy(t):
        at = block(0) if t == 0 else pl.ds(rows, count - rows)
        return pltpu.make_async_copy(leak.at[at], cums.at[at], leak_sem.at[t])

    weights = ((wf, 0, 0), (wi, 0, 1), (wc, 1, 0), (wh, 1, 1), (wb, 1, 2), (wq, 2, 0), (wg, 2, 1))
    weight_sems = (0, 0, 1, 2, 3, 4, 4)

    phases = [w_scan, w_conv, w_read]

    def weight_copy(n):
        src, phase, slot = weights[n]
        dst = phases[phase]
        return pltpu.make_async_copy(
            src, dst.at[:, slot * width : (slot + 1) * width], w_sem.at[weight_sems[n]]
        )

    def weight_wait(phase):
        dst = phases[phase]
        pltpu.make_async_copy(dst, dst, w_sem.at[weight_sems[2 * phase + phase // 2]]).wait()

    def cols_of(device):
        return pl.ds(pl.multiple_of(device * ncols, ncols), ncols)

    def piece_rows(g):
        return pl.ds(pl.multiple_of(g * piece, piece), piece)

    def own_columns(kind):
        return pltpu.make_async_copy(
            outs[kind].at[:, cols_of(me)], columns.at[kind, me], own_sem.at[0]
        )

    def pair_columns(kind, origin):
        return pltpu.make_async_remote_copy(
            outs[kind].at[:, cols_of(partner)], columns.at[kind, origin],
            pair_send.at[0], pair_recv.at[0], device_id={"tp": partner},
        )

    def far(k, c):
        return lax.rem(chip + k, chips) * 2 + c

    def piece_out(kind, k, c):
        target = far(k, c)
        return pltpu.make_async_remote_copy(
            outs[kind].at[piece_rows(mine), cols_of(target)],
            columns.at[kind, me, piece_rows(mine)],
            piece_send.at[0], piece_recv.at[kind, chips - k - 1, core, 0],
            device_id={"tp": target},
        )

    def piece_in(kind, k, c, n):
        ref = columns.at[kind, me, 0:piece]
        return pltpu.make_async_copy(ref, ref, piece_recv.at[kind, k - 1, c, n])

    def pass_on(kind, k, c, n):
        g, to = ((mine, mate), (mine, twin), (mates_piece, twin))[n]
        ref = columns.at[kind, far(k, c), piece_rows(g)]
        return pltpu.make_async_remote_copy(
            ref, ref, mate_send.at[0],
            piece_recv.at[kind, k - 1, c, 1] if n == 0 else twin_recv.at[0],
            device_id={"sp": to},
        )

    def pieces_wait(n, sem):
        ref = columns.at[:, 0 : tp - 2, 0 : n * piece]
        pltpu.make_async_copy(ref, ref, sem.at[0]).wait()

    def pass_own(kind, wait, which):
        for k, c in far_devices:
            if wait:
                piece_in(kind, k, c, 0).wait()
            for n in which:
                pass_on(kind, k, c, n).start()

    def pass_mates(kind):
        for k, c in far_devices:
            piece_in(kind, k, c, 1).wait()
            pass_on(kind, k, c, 2).start()

    far_devices = [(k, c) for k in range(1, chips) for c in range(2)]

    def span(kind, t):
        if kind == CONV and isinstance(t, int):
            if t == 0:
                return pl.ds(HEAD, rows - HEAD)
            if t == nb:
                return pl.ds(0, HEAD)
        return mix_block(t) if kind == MIX else block(t)

    def recv_sem(kind, slot, t):
        return conv_recv.at[slot] if kind == CONV or slot == 0 else mix_recv.at[slot - 1, t]

    def first_recv(kind):
        return (conv_recv if kind == CONV else mix_first).at[0]

    def own_copies(kind, t):
        ref = held[kind].at[me, span(kind, t)]
        out = []
        for k in range(1, chips):
            out.append(pltpu.make_async_remote_copy(
                ref, ref, blk_send.at[kind, k], recv_sem(kind, chips - k, t),
                device_id={"tp": far(k, core)},
            ))
        out.append(pltpu.make_async_remote_copy(
            ref, ref, blk_send.at[kind, 0], first_recv(kind), device_id={"tp": partner}
        ))
        return out

    def relays(kind, t):
        out = []
        for k in range(1, chips):
            ref = held[kind].at[far(k, core)]
            if kind == MIX:
                ref = ref.at[mix_block(t)]
            out.append(pltpu.make_async_remote_copy(
                ref, ref, fwd_send.at[kind, k - 1], recv_sem(kind, chips - 1 + k, t),
                device_id={"tp": partner},
            ))
        return out

    def start(copies):
        for copy in copies:
            copy.start()

    def landed(kind, slot, t):
        ref = held[kind].at[me]
        if kind == MIX:
            ref = ref.at[mix_block(t)]
        pltpu.make_async_copy(ref, ref, recv_sem(kind, slot, t)).wait()

    def relay(kind, t):
        for k, copy in enumerate(relays(kind, t)):
            landed(kind, k + 1, t)
            copy.start()

    def first_landed(kind):
        ref = held[kind].at[me]
        pltpu.make_async_copy(ref, ref, first_recv(kind)).wait()

    def sent(kind):
        ref = held[kind].at[me]
        for k in range(chips):
            pltpu.make_async_copy(ref, ref, blk_send.at[kind, k]).wait()

    def passed_on(kind):
        ref = held[kind].at[me]
        for k in range(1, chips):
            pltpu.make_async_copy(ref, ref, fwd_send.at[kind, k - 1]).wait()

    def twin_copy(h):
        return pltpu.make_async_remote_copy(
            sent_state.at[h], peer_state.at[h], l1_send.at[0], l1_recv.at[h],
            device_id={"sp": twin},
        )

    def total_copy(k, source, h):
        return pltpu.make_async_remote_copy(
            sent_total.at[h], totals.at[source, h], l2_send.at[k - 1], l2_recv.at[source],
            device_id={"sp": lax.rem(place + 2 * k, sp)},
        )

    def put_decay(ref, h, decay):
        high = decay.astype(bf16)
        low = (decay - high.astype(f32)).astype(bf16)
        both = jnp.concatenate([high, low], axis=0)
        ref[h, GROUP_FEATURES:, :] = jnp.concatenate([both] * (EXTRA // 2), axis=0)

    def decay_of(rows_of):
        both = rows_of.astype(f32)
        return both[0:1] + both[1:2]

    rim_copy = pltpu.make_async_remote_copy(
        tail, rim, rim_send.at[0], rim_recv.at[0], device_id={"sp": after}
    )

    small = ((in_gain_in, in_gain), (floor_in, floor), (state_gain_in, state_gain),
             (taps_in, taps), (group_gain_in, group_gain))

    def small_copy(n):
        return pltpu.make_async_copy(small[n][0], small[n][1], small_sem.at[n])

    small_copy(0).start()
    token_copy(0).start()
    weight_copy(0).start()
    weight_copy(1).start()
    small_copy(1).start()
    leak_copy(0).start()
    if nb > 1:
        token_copy(1).start()
        leak_copy(1).start()
    barrier = pltpu.get_barrier_semaphore()
    for k in range(1, tp):
        pl.semaphore_signal(barrier, inc=1, device_id={"tp": lax.rem(me + k, tp)})
    for to, low in ((twin, member == 0), (mate, step > 0)):
        @pl.when(low)
        def _():
            pl.semaphore_signal(barrier, inc=1, device_id={"sp": to})

    for k in range(1, pairs):
        @pl.when(pair + k < pairs)
        def _():
            pl.semaphore_signal(barrier, inc=1, device_id={"sp": lax.rem(place + 2 * k, sp)})
    follows = jnp.logical_and(member == 0, pair > 0)
    leads = jnp.logical_and(member == 1, pair < pairs - 1)

    @pl.when(leads)
    def _():
        pl.semaphore_signal(barrier, inc=1, device_id={"sp": after})

    lower = pair + member + jnp.where(step > 0, 0, 1) + jnp.where(follows, 1, 0)
    pl.semaphore_wait(barrier, tp - 1 + lower)

    @pl.when(member == 1)
    def _():
        pl.semaphore_signal(twin_ready, inc=1, device_id={"sp": twin})

    @pl.when(step < 0)
    def _():
        pl.semaphore_signal(mate_ready, inc=1, device_id={"sp": mate})

    for k in range(1, pairs):
        @pl.when(pair >= k)
        def _():
            pl.semaphore_signal(ready, inc=1, device_id={"sp": lax.rem(place + sp - 2 * k, sp)})

    @pl.when(follows)
    def _():
        pl.semaphore_signal(rim_ready, inc=1, device_id={"sp": before})
    for kind in (CONV, MIX):
        for k, c in far_devices:
            piece_out(kind, k, c).start()
    for t in range(2, nb):
        token_copy(t).start()
    for n in (2, 3, 4):
        weight_copy(n).start()
    for n in (2, 3, 4):
        small_copy(n).start()
    for kind in (CONV, MIX):
        pair_columns(kind, me).start()
        own_columns(kind).start()

    state[...] = jnp.zeros_like(state)
    offset[...] = jnp.zeros_like(offset)
    pad[0:HALO, :] = jnp.zeros((HALO, channels), f32)

    r = lax.broadcasted_iota(jnp.int32, (CHUNK, CHUNK), 0)
    c = lax.broadcasted_iota(jnp.int32, (CHUNK, CHUNK), 1)
    causal = r >= c
    ones = jnp.concatenate([causal.astype(f32)] * 3, axis=1).astype(bf16)

    def arrive(t):
        token_copy(t).wait()
        if t < 2:
            leak_copy(t).wait()

    def norm(t):
        arrive(t)
        normalize(t)

    def normalize(t):
        at = block(t)
        normed_all[at, :] = (rms(normed_all[at, :].astype(f32)) * in_gain[...]).astype(bf16)

    def scan_product(t):
        return dot(normed_all[block(t), :], w_scan[...])

    def scan_block(t, both):
        at = block(t)
        x = both[:, :width].astype(bf16).astype(f32)
        value = both[:, width:].astype(bf16)
        value_all[at, :] = value
        key = (1.0 - floor[...]) * jax.nn.sigmoid(-x)
        logf = jnp.log(1.0 - key) + cums[at, :]
        for b in range(rows // CHUNK):
            lo, hi = b * CHUNK, (b + 1) * CHUNK
            where = pl.ds(t * rows + lo, CHUNK)
            number = t * (rows // CHUNK) + b
            cum = prefix_sum(ones, logf[lo:hi])
            mid = cum[CHUNK // 2 - 1 : CHUNK // 2]
            last = cum[CHUNK - 1 : CHUNK]
            k_mid = key[lo:hi] * jnp.exp(mid - cum)
            k_end = (k_mid * jnp.exp(last - mid)).astype(bf16)
            cums[where, :] = cum
            key_mid[where, :] = k_mid.astype(bf16)
            offsets[number] = offset[...]
            for h in range(heads):
                s = head_slice(h)
                old = state[h]
                olds[number, h] = old.astype(bf16)
                state[h] = old * jnp.exp(last[:, s]) + dot(
                    value[lo:hi, s], k_end[:, s], ((0,), (0,))
                )
            offset[...] += last

    def conv_third(n):
        return dot(normed_all[block(0), :], w_conv[:, n * channels : (n + 1) * channels])


    def conv_product(t):
        return dot(normed_all[block(t), :], w_conv[...])

    def conv_block(t, three):
        at = block(t)
        first = three[:, :channels].astype(bf16).astype(f32)
        second = three[:, channels : 2 * channels].astype(bf16).astype(f32)
        proj_b = three[:, 2 * channels :].astype(bf16).astype(f32)
        conv_in = (first * second).astype(bf16).astype(f32)
        w_taps = taps[...].astype(f32)
        pad[HALO : HALO + rows, :] = conv_in
        total = w_taps[TAPS - 1 : TAPS] * conv_in
        for j in range(TAPS - 1):
            lo = HALO - (TAPS - 1) + j
            total += w_taps[j : j + 1] * pad[lo : lo + rows, :]
        conv_all[me, at, :] = per_group(proj_b * total, group_gain[...]).astype(bf16)

        @pl.when(t == 0)
        def _():
            head_conv[...] = conv_in[:HALO]
            head_gate[...] = proj_b[:HALO]
            start(own_copies(CONV, 0))

        @pl.when(t > 0)
        def _():
            start(own_copies(CONV, t))

        pad[0:HALO, :] = conv_in[rows - HALO :]

        @pl.when(t == nb - 1)
        def _():
            tail[...] = conv_in[rows - HALO :]

            @pl.when(leads)
            def _():
                pl.semaphore_wait(rim_ready, 1)

            @pl.when(place < sp - 1)
            def _():
                rim_copy.start()

            pass_own(MIX, True, (1,))

            @pl.when(step < 0)
            def _():
                pass_own(MIX, False, (0,))


        @pl.when(t == nb - 1)
        def _():
            @pl.when(pair < pairs - 1)
            def _():
                pl.semaphore_wait(ready, pairs - 1 - pair)

            for h in range(heads):
                s = head_slice(h)
                twin_copy(h).wait_recv()
                own, other = state[h], peer_state[h, :GROUP_FEATURES, :].astype(f32)
                own_decay = jnp.exp(offset[0:1, s])
                peer_decay = decay_of(peer_state[h, GROUP_FEATURES:, :])
                early = jnp.where(member == 0, own, other)
                late = jnp.where(member == 0, other, own)
                decay = jnp.where(member == 0, peer_decay, own_decay)
                sent_total[h, :GROUP_FEATURES, :] = (early * decay + late).astype(bf16)
                put_decay(sent_total, h, own_decay * peer_decay)
                for k in reversed(range(1, pairs)):
                    @pl.when(pair + k < pairs)
                    def _():
                        total_copy(k, pair, h).start()

    conv_thirds = []
    small_copy(0).wait()
    norm(0)
    small_copy(1).wait()
    weight_wait(0)
    for n in (5, 6):
        weight_copy(n).start()
    product = scan_product(0)
    if nb > 1:
        norm(1)
    for t in range(nb):
        if t + 2 < nb:
            arrive(t + 2)
        thirds = [n for n in range(3) if t == max(nb - 4 + min(n, 1), 0)]
        for n in thirds:
            weight_copy(2 + n).wait()
        if t + 1 < nb:
            later = scan_product(t + 1)
        for n in thirds:
            conv_thirds.append(conv_third(n))
        if t + 2 < nb:
            normalize(t + 2)
        if t == max(nb - 2, 0):
            for n in (2, 3, 4):
                small_copy(n).wait()
            conv_block(0, jnp.concatenate(conv_thirds, axis=1))
        scan_block(t, product)
        product = later
    sent_state[:, :GROUP_FEATURES, :] = state[...].astype(bf16)
    for h in range(heads):
        put_decay(sent_state, h, jnp.exp(offset[0:1, head_slice(h)]))

    @pl.when(member == 0)
    def _():
        pl.semaphore_wait(twin_ready, 1)

    for h in range(heads):
        twin_copy(h).start()

    @pl.when(step > 0)
    def _():
        pl.semaphore_wait(mate_ready, 1)

    pass_own(CONV, True, (0, 1))

    if nb > 1:
        product = conv_product(1)
    for t in range(1, nb):
        if t + 1 < nb:
            later = conv_product(t + 1)
        conv_block(t, product)
        product = later

    weight_wait(2)

    def read_product(t):
        return dot(normed_all[block(t), :], w_read[...])

    def read_block(t, both):
        at = block(t)
        query = jax.nn.silu(both[:, :width].astype(bf16).astype(f32))
        outgate = jax.nn.silu(both[:, width:].astype(bf16).astype(f32))
        for h in range(heads):
            s = head_slice(h)
            gate[at, s] = outgate[:, s] * state_gain[...]
        for b in range(rows // CHUNK):
            lo, hi = b * CHUNK, (b + 1) * CHUNK
            where = pl.ds(t * rows + lo, CHUNK)
            number = t * (rows // CHUNK) + b
            cum = cums[where, :]
            mid = cum[CHUNK // 2 - 1 : CHUNK // 2]
            q_mid = query[lo:hi] * jnp.exp(cum - mid)
            q_all = q_mid * jnp.exp(mid)
            qdev[where, :] = (q_all * jnp.exp(offsets[number, 0:1, :])).astype(bf16)
            q_mid, q_all = q_mid.astype(bf16), q_all.astype(bf16)
            for h in range(heads):
                s = head_slice(h)
                scores = dot(q_mid[:, s], key_mid[where, s], ((1,), (1,)))
                scores = jnp.where(causal, scores, 0.0).astype(bf16)
                read[where, s] = dot(scores, value_all[where, s]) + dot(
                    q_all[:, s], olds[number, h], ((1,), (1,))
                )

        if t == nb // 2:
            pass_mates(CONV)

        @pl.when(t == nb - 1)
        def _():
            @pl.when(place == 0)
            def _():
                rim[...] = jnp.zeros_like(rim)

            @pl.when(place > 0)
            def _():
                rim_copy.wait_recv()

            ext = jnp.concatenate([rim[...], head_conv[...]], axis=0)
            w_taps = taps[...].astype(f32)
            fixed = w_taps[TAPS - 1 : TAPS] * head_conv[...]
            for j in range(TAPS - 1):
                lo = HALO - (TAPS - 1) + j
                fixed += w_taps[j : j + 1] * ext[lo : lo + HALO]
            fixed = per_group(head_gate[...] * fixed, group_gain[...])
            conv_all[me, 0:HALO, :] = fixed.astype(bf16)
            start(own_copies(CONV, nb))

            @pl.when(step > 0)
            def _():
                pass_own(MIX, False, (0,))
                pass_mates(MIX)


    product = read_product(0)
    for t in range(nb):
        if t + 1 < nb:
            later = read_product(t + 1)
        read_block(t, product)
        product = later

    for k in range(1, pairs):
        @pl.when(pair >= k)
        def _():
            ref = totals.at[pair - k]
            pltpu.make_async_copy(ref, ref, l2_recv.at[pair - k]).wait()
    incoming[...] = jnp.zeros_like(incoming)

    def hop(p, _):
        for h in range(heads):
            decay = decay_of(totals[p, h, GROUP_FEATURES:, :])
            incoming[h] = incoming[h] * decay + totals[p, h, :GROUP_FEATURES, :].astype(f32)
        return 0

    lax.fori_loop(0, pair, hop, 0)
    for h in range(heads):
        decay = decay_of(peer_state[h, GROUP_FEATURES:, :])
        through = incoming[h] * decay + peer_state[h, :GROUP_FEATURES, :].astype(f32)
        incoming[h] = jnp.where(member == 0, incoming[h], through)

    def merge(t, _):
        at = block(t)
        for h in range(heads):
            s = head_slice(h)
            whole = read[at, s] + dot(qdev[at, s], incoming[h].astype(bf16), ((1,), (1,)))
            mix_all[me, at, s] = (rms(whole) * gate[at, s]).astype(bf16)
        for n in range(rows // MIX_ROWS):
            start(own_copies(MIX, t * (rows // MIX_ROWS) + n))
        return 0

    lax.fori_loop(0, nb, merge, 0)

    mine_both, pair_both = columns.at[:, me], columns.at[:, partner]
    pltpu.make_async_copy(mine_both, mine_both, own_sem.at[0]).wait()
    pltpu.make_async_copy(pair_both, pair_both, pair_recv.at[0]).wait()

    def near(kind, t):
        out = dot(held[kind][me, block(t), :], columns[kind, me])
        return out + dot(held[kind][partner, block(t), :], columns[kind, partner])

    def near_conv(t, _):
        acc_all[block(t), :] = near(CONV, t)
        return 0

    first_landed(CONV)
    lax.fori_loop(0, nb, near_conv, 0)

    def near_mix(t, _):
        acc_all[block(t), :] += near(MIX, t)
        return 0

    first_landed(MIX)
    lax.fori_loop(0, nb, near_mix, 0)

    @pl.when(step < 0)
    def _():
        pass_mates(MIX)

    relay(CONV, 0)

    pieces_wait(2, twin_recv)
    for k in range(1, chips):
        landed(CONV, chips - 1 + k, 0)

    def far_conv(t, _):
        acc = acc_all[block(t), :]
        for k, c in far_devices:
            origin = far(k, c)
            acc += dot(conv_all[origin, block(t), :], columns[CONV, origin])
        acc_all[block(t), :] = acc
        return 0

    lax.fori_loop(0, nb, far_conv, 0)

    sent(CONV)
    passed_on(CONV)
    pieces_wait(1, piece_send)
    pieces_wait(3, mate_send)
    pltpu.make_async_copy(mine_both, mine_both, pair_send.at[0]).wait()

    @pl.when(place < sp - 1)
    def _():
        rim_copy.wait_send()

    pltpu.make_async_copy(sent_state, sent_state, l1_send.at[0]).wait()
    for k in range(1, pairs):
        @pl.when(pair + k < pairs)
        def _():
            pltpu.make_async_copy(sent_total, sent_total, l2_send.at[k - 1]).wait()

    def finish(t, _):
        @pl.when(t + LAG < mix_nb)
        def _():
            relay(MIX, t + LAG)

        for k in range(1, chips):
            landed(MIX, chips - 1 + k, t)
        at = mix_block(t)
        acc = acc_all[at, :]
        for k, c in far_devices:
            origin = far(k, c)
            acc += dot(mix_all[origin, at, :], columns[MIX, origin])
        result[at, :] = acc.astype(bf16)
        return 0

    for t in range(min(LAG, mix_nb)):
        relay(MIX, t)
    lax.fori_loop(0, mix_nb, finish, 0)

    sent(MIX)
    passed_on(MIX)


def body(
    tokens, in_gain, w_query, w_forget, w_input, w_outgate, w_conv_h, w_conv_b, w_conv_c,
    forget_floor, forget_leak, state_gain, conv_taps, group_gain, out_state, out_conv,
):
    count, feats = tokens.shape
    width, channels = w_query.shape[1], w_conv_h.shape[1]
    heads = width // GROUP_FEATURES
    tp, sp = lax.axis_size("tp"), lax.axis_size("sp")
    ncols, nb, chips = out_state.shape[1] // tp, count // ROWS, tp // 2
    share = min(SHARE, sp)
    chunks, pairs = count // CHUNK, sp // 2

    hbm = pl.BlockSpec(memory_space=pltpu.HBM)
    vmem = pl.BlockSpec(memory_space=pltpu.VMEM)
    sems = pltpu.SemaphoreType.DMA
    square = (heads, GROUP_FEATURES, GROUP_FEATURES)
    longer = (heads, GROUP_FEATURES + EXTRA, GROUP_FEATURES)
    return pl.pallas_call(
        functools.partial(fused_kernel, tp, sp, share),
        in_specs=[hbm] * 16,
        out_specs=vmem,
        out_shape=pltpu.VMEM((count, ncols), bf16),
        scratch_shapes=[
            pltpu.VMEM((1, feats), f32),
            pltpu.VMEM((1, width), f32),
            pltpu.VMEM((1, GROUP_FEATURES), f32),
            pltpu.VMEM((TAPS, channels), bf16),
            pltpu.VMEM((1, GROUP_FEATURES), f32),
            sems((5,)),
            pltpu.VMEM((count, feats), bf16),
            pltpu.VMEM((feats, 2 * width), bf16),
            pltpu.VMEM((feats, 3 * channels), bf16),
            pltpu.VMEM((feats, 2 * width), bf16),
            pltpu.VMEM((count, width), f32),
            pltpu.VMEM((count, width), bf16),
            pltpu.VMEM((count, width), bf16),
            pltpu.VMEM((chunks,) + square, bf16),
            pltpu.VMEM((chunks, HALO, width), f32),
            pltpu.VMEM((HALO + ROWS, channels), f32),
            pltpu.VMEM(square, f32),
            pltpu.VMEM((HALO, width), f32),
            pltpu.VMEM((count, width), f32),
            pltpu.VMEM((count, width), bf16),
            pltpu.VMEM((count, width), f32),
            pltpu.VMEM((tp, count, channels), bf16),
            pltpu.VMEM((tp, count, width), bf16),
            pltpu.VMEM((2, tp, width, ncols), bf16),
            pltpu.VMEM((count, ncols), f32),
            pltpu.VMEM(longer, bf16),
            pltpu.VMEM(longer, bf16),
            pltpu.VMEM(longer, bf16),
            pltpu.VMEM((pairs,) + longer, bf16),
            pltpu.VMEM((HALO, channels), f32),
            pltpu.VMEM((HALO, channels), f32),
            pltpu.VMEM((HALO, channels), f32),
            pltpu.VMEM((HALO, channels), f32),
            pltpu.VMEM(square, f32),
            sems((nb,)), sems((2,)), sems((5,)), sems((1,)),
            sems((1,)), sems((1,)), sems((1,)), sems((2, chips - 1, 2, 2)), sems((1,)), sems((1,)),
            sems((2, chips)), sems((2, chips - 1)), sems((2 * chips - 1,)), sems((1,)),
            sems((2 * chips - 2, count // MIX_ROWS)),
            sems((1,)), sems((heads,)), sems((pairs - 1,)), sems((pairs - 1,)),
            sems((1,)), sems((1,)),
        ] + [pltpu.SemaphoreType.REGULAR] * 4,
        compiler_params=pltpu.CompilerParams(
            vmem_limit_bytes=56 * 2**20, collective_id=0, has_side_effects=True
        ),
    )(
        tokens, in_gain[None], w_query, w_forget, w_input, w_outgate, w_conv_h, w_conv_b, w_conv_c,
        forget_floor[None], forget_leak, state_gain[None], conv_taps, group_gain[None],
        out_state, out_conv,
    )


def solution(mesh):
    cols, rows = P(None, "tp"), P("tp", None)
    in_specs = (
        P("sp", None), P(), cols, cols, cols, cols, cols, cols, cols,
        P("tp"), P("sp", "tp"), P(), cols, P(), rows, rows,
    )
    return jax.shard_map(
        body, mesh=mesh, in_specs=in_specs, out_specs=P("sp", "tp"), check_vma=False
    )
```
